256 devices in a mesh: ep: 16 (over y, x), tp: 16 (over z, core).
Axes of the slice: x: 4, y: 4, z: 8, core: 2. Of those that a mesh axis runs over, the one named last changes fastest.
Arguments:
- tokens: bfloat16 [1024, 2048], P('ep', 'tp'), may hold values from -6 to 6
- prior_state: float32 [1024, 16, 64, 128], P('ep', 'tp'), may hold values from -3 to 3
- decay_rate: float32 [16], P('tp'), may hold values from 0.01 to 0.5
- norm_in: float32 [2048], replicated, may hold values from 0.1 to 1.9
- query_weight: bfloat16 [2048, 1024], P(None, 'tp'), may hold values from -0.125 to 0.125
- key_weight: bfloat16 [2048, 1024], P(None, 'tp'), may hold values from -0.125 to 0.125
- value_weight: bfloat16 [2048, 2048], P(None, 'tp'), may hold values from -0.125 to 0.125
- gate_weight: bfloat16 [2048, 2048], P(None, 'tp'), may hold values from -0.125 to 0.125
- out_weight: bfloat16 [2048, 2048], P('tp'), may hold values from -0.125 to 0.125
- norm_moe: float32 [2048], replicated, may hold values from 0.1 to 1.9
- routes: int32 [1024, 2], replicated, may hold values from 0 to 15, all different within a row; in each aligned block of 64 rows (0 to 63, 64 to 127, ...) at most 12 rows name the same one
- route_weight: float32 [1024, 2], replicated, may hold values from 0.1 to 1
- expert_gate: bfloat16 [16, 2048, 7168], P('ep', None, 'tp'), may hold values from -0.125 to 0.125
- expert_up: bfloat16 [16, 2048, 7168], P('ep', None, 'tp'), may hold values from -0.125 to 0.125
- expert_down: bfloat16 [16, 7168, 2048], P('ep', 'tp'), may hold values from -0.0625 to 0.0625
Outputs:
- next_hidden: bfloat16 [1024, 2048], P('ep', 'tp')
- new_state: float32 [1024, 16, 64, 128], P('ep', 'tp')
The draws below stay inside these ranges and needn't reach their ends.
Inputs may be any that keep to these rules, and one draw needn't show every extreme that they name: `routes`: the 2 experts of a row differ. In each aligned block of 64 rows (the sequences of one index of ep), no expert is named by more than 12 rows, a bound that some block reaches.
All inputs are finite; a program needn't handle non-finite values.
Results may differ from the reference program's by a relative error of at most 0.011.
Values may be sent and summed in bfloat16 or wider, within the bound.
A program may use at most 64 MiB of HBM per device.

```python
import math
import jax
import jax.numpy as jnp
import numpy as np
from jax import lax

D = 2048
HEADS = 16
DK = 64
DV = 128
FFE = 7168
TOP_K = 2
SEQ_DEV = 64
EXPERTS = 16
CAP = 12
BATCH = 1024
HK = 1024
HV = 2048
N_EP = 16


def block_levels(key, dims, shards, low, top_value):
    factor_of = 1.0
    for axis_at, parts in shards:
        steps = jax.random.uniform(jax.random.fold_in(jax.random.fold_in(key, 6), axis_at), (parts,), jnp.float32, low / len(shards), top_value / len(shards))
        factor_of = factor_of * jnp.repeat(jnp.exp(steps), dims[axis_at] // parts).reshape((-1,) + (1,) * (len(dims) - 1 - axis_at))
    return factor_of


def routed_block(stream_key, own, number, rows, amount, top, reach, slope):
    order = jax.random.permutation(stream_key, amount)
    packed, ordinary = shares(amount, rows * top, reach, slope, True), shares(amount, rows * top, reach, slope, False)
    places = jnp.arange(amount)

    def named(lengths, offset_by):
        used = int((lengths > 0).sum())
        fixed = max(1, used // 4)
        passed = fixed + (places - fixed + offset_by * (used - fixed)) % max(1, amount - fixed)
        return jnp.zeros((amount,), jnp.int32).at[order[jnp.where(places < fixed, places, passed)]].set(jnp.asarray(lengths, jnp.int32))

    lengths = jnp.where(number % 4 == 0, named(packed, number // 4), named(ordinary, number - number // 4 - 1))
    mixed = jax.random.permutation(jax.random.fold_in(own, 3), amount)
    giver, sink = mixed[0:amount // 2 * 2:2], mixed[1:amount // 2 * 2:2]
    slack = jnp.minimum(lengths[giver] - 1, reach - lengths[sink]) // 2
    slack = jnp.where((giver == order[0]) | (sink == order[0]) | (lengths[sink] == 0), 0, jnp.maximum(slack, 0))
    passed = jax.random.randint(jax.random.fold_in(own, 4), (amount // 2,), 0, 1 << 20) % (slack + 1)
    lengths = lengths.at[giver].add(-passed).at[sink].add(passed)
    items = jnp.searchsorted(jnp.cumsum(lengths), jnp.arange(rows * top), side="right").astype(jnp.int32)
    listing = items.reshape(top, rows).T
    listing = listing[jax.random.permutation(jax.random.fold_in(own, 1), rows)]
    offset_by = jax.random.randint(jax.random.fold_in(own, 2), (rows, 1), 0, top)
    return jnp.take_along_axis(listing, (jnp.arange(top)[None, :] + offset_by) % top, axis=1)


def shares(number_of, total, limit, skew, full):
    portions = [(1 << 20) // math.isqrt(grade ** skew) + 1 for grade in range(1, number_of + 1)]
    largest = limit if full else min(limit, max(-(-total // number_of), total * portions[0] // sum(portions)))
    least = 1 if total - largest >= number_of - 1 else 0
    counts, surplus = [largest] + [least] * (number_of - 1), total - largest - least * (number_of - 1)
    while surplus > 0:
        free = [i for i in range(1, number_of) if counts[i] < largest] or [i for i in range(1, number_of) if counts[i] < limit]
        whole, budget = sum([portions[i] for i in free]), surplus
        for i in free:
            more = min(limit - counts[i], max(1, budget * portions[i] // whole), surplus)
            counts[i] = counts[i] + more
            surplus = surplus - more
    return np.array(counts)


def noise(key, dims, spread, limit, shards=(), kind=jnp.bfloat16):
    drawn = jax.random.normal(key, dims, jnp.float32) * spread
    if len(shards) > 0:
        drawn = block_levels(key, dims, shards, -0.22, 0.18) * drawn
    return jnp.clip(drawn, min=-limit, max=limit).astype(kind)


def setup_inputs(seed: int = 0) -> dict:
    keys = jax.random.split(jax.random.key(seed), 16)
    tokens = noise(keys[0], (BATCH, D), 1.0, 6.0, ((0, 16), (1, 16)))
    prior_state = noise(keys[1], (BATCH, HEADS, DK, DV), 0.5, 3.0, ((0, 16), (1, 16)), jnp.float32)
    decay_rate = jnp.clip(jnp.exp(math.log(0.5) - 3.912023 * jax.random.uniform(keys[2], (HEADS,), jnp.float32) ** block_levels(keys[2], (HEADS,), ((0, 16),), -0.2, 0.2)), 0.01, 0.5)
    norm_in = jnp.clip(1.0 + 0.18 * jax.random.normal(keys[3], (D,), jnp.float32), 0.1, 1.9)
    query_weight = noise(keys[4], (D, HK), D ** -0.5, 0.125, ((1, 16),))
    key_weight = noise(keys[5], (D, HK), D ** -0.5, 0.125, ((1, 16),))
    value_weight = noise(keys[6], (D, HV), D ** -0.5, 0.125, ((1, 16),))
    gate_weight = noise(keys[7], (D, HV), D ** -0.5, 0.125, ((1, 16),))
    out_weight = noise(keys[8], (HV, D), HV ** -0.5, 0.125, ((0, 16),))
    norm_moe = jnp.clip(1.0 + 0.18 * jax.random.normal(keys[9], (D,), jnp.float32), 0.1, 1.9)
    routes_keys = jax.random.split(jax.random.fold_in(keys[10], 1), BATCH // SEQ_DEV)
    routes_turns = jax.random.permutation(jax.random.fold_in(keys[10], 3), BATCH // SEQ_DEV)
    routes = jax.vmap(lambda own, number: routed_block(jax.random.fold_in(keys[10], 2), own, number, SEQ_DEV, EXPERTS, TOP_K, CAP, 2))(routes_keys, routes_turns).reshape((BATCH, TOP_K))
    route_weight = jnp.clip(jax.random.uniform(keys[11], (BATCH, TOP_K), jnp.float32, 0.1, 1.0), 0.1, 1.0)
    expert_gate = noise(keys[12], (EXPERTS, D, FFE), D ** -0.5, 0.125, ((0, 16), (2, 16)))
    expert_up = noise(keys[13], (EXPERTS, D, FFE), D ** -0.5, 0.125, ((0, 16), (2, 16)))
    expert_down = noise(keys[14], (EXPERTS, FFE, D), FFE ** -0.5, 0.0625, ((0, 16), (1, 16)))
    return dict(tokens=tokens, prior_state=prior_state, decay_rate=decay_rate, norm_in=norm_in, query_weight=query_weight, key_weight=key_weight, value_weight=value_weight, gate_weight=gate_weight, out_weight=out_weight, norm_moe=norm_moe, routes=routes, route_weight=route_weight, expert_gate=expert_gate, expert_up=expert_up, expert_down=expert_down)


EPSILON = 1e-06

def rms_scale(row_block, gain_row):
    values = row_block.astype(jnp.float32)
    factor = lax.rsqrt(lax.optimization_barrier(jnp.mean(values * values, -1, keepdims=True)) + EPSILON)
    return (values * factor * gain_row).astype(jnp.bfloat16)

def project(normed_in, weight):
    stored = jnp.dot(normed_in, weight, preferred_element_type=jnp.float32).astype(jnp.bfloat16)
    return lax.optimization_barrier(stored).astype(jnp.float32)

def reference(tokens, prior_state, decay_rate, norm_in, query_weight, key_weight, value_weight, gate_weight, out_weight, norm_moe, routes, route_weight, expert_gate, expert_up, expert_down):
    total = tokens.shape[0]
    normed_in = rms_scale(tokens, norm_in)
    query = project(normed_in, query_weight).reshape(total, HEADS, DK)
    keyed = project(normed_in, key_weight).reshape(total, HEADS, DK) * DK ** (-0.5)
    valued = project(normed_in, value_weight).reshape(total, HEADS, DV)
    gate_pre = project(normed_in, gate_weight)
    keep = (1.0 - decay_rate)[None, :, None, None]
    new_state = keep * prior_state + jnp.einsum('bhk,bhv->bhkv', keyed, valued, precision=lax.Precision.HIGHEST)
    read = jnp.einsum('bhk,bhkv->bhv', query, new_state, precision=lax.Precision.HIGHEST)
    centred = read - lax.optimization_barrier(jnp.mean(read, -1, keepdims=True))
    normed = centred * lax.rsqrt(lax.optimization_barrier(jnp.mean(centred * centred, -1, keepdims=True)) + EPSILON)
    mixed_heads = (jax.nn.silu(gate_pre) * normed.reshape(total, HEADS * DV)).astype(jnp.bfloat16)
    mixer_out = jnp.dot(mixed_heads, out_weight, preferred_element_type=jnp.float32)
    resid = (tokens.astype(jnp.float32) + mixer_out).astype(jnp.bfloat16)
    expert_in = rms_scale(resid, norm_moe)
    slot_count = N_EP * CAP
    slot_ids = jnp.arange(slot_count, dtype=jnp.int32)

    def one_expert(carry, pack):
        label, gate_w, up_w, down_w = pack
        match = routes == label
        chosen = lax.optimization_barrier(jnp.sum(match.astype(jnp.int32), 1)).astype(jnp.int32)
        weighted = lax.optimization_barrier(jnp.sum(jnp.where(match, route_weight, 0.0), 1))
        rank = jnp.cumsum(chosen).astype(jnp.int32) - chosen
        place = ((rank[:, None] == slot_ids[None, :]) & (chosen[:, None] > 0)).astype(jnp.float32)
        rows_in = jnp.dot(place.T.astype(jnp.bfloat16), expert_in, preferred_element_type=jnp.float32).astype(jnp.bfloat16)
        gate_part = jnp.dot(rows_in, gate_w, preferred_element_type=jnp.float32)
        up_part = jnp.dot(rows_in, up_w, preferred_element_type=jnp.float32)
        hidden = (jax.nn.silu(gate_part) * up_part).astype(jnp.bfloat16)
        down = jnp.dot(hidden, down_w, preferred_element_type=jnp.float32)
        carry = carry + jnp.dot(place * weighted[:, None], down, precision=lax.Precision.HIGHEST)
        return (carry, None)
    start = jnp.zeros((total, D), jnp.float32)
    labels = jnp.arange(EXPERTS, dtype=jnp.int32)
    moe_sum, unused = lax.scan(one_expert, start, (labels, expert_gate, expert_up, expert_down))
    next_hidden = (resid.astype(jnp.float32) + moe_sum).astype(jnp.bfloat16)
    return (next_hidden, new_state)
```

```python
import functools
import jax
import jax.numpy as jnp
from jax import lax
from jax.experimental import pallas as pl
from jax.experimental.pallas import tpu as pltpu
from jax.sharding import PartitionSpec as P

DK = 64
DV = 128
SLOT = 16
EPSILON = 1e-06
F32 = jnp.float32
BF16 = jnp.bfloat16


def near_first(n):
    return sorted(range(1, n), key=lambda d: (min(d, n - d), d))


def layer_kernel(
    nx, ny, nz, cap,
    tokens, prior, decay_in, norm_in, wq, wk, wv, wg, wo, norm_moe,
    routes, route_w, egate, eup, edown,
    out, k_out, v_out,
    decay, tok, wqk_v, wv_v, wg_v, prior_v, nin_v, nmoe_v, rt_v, rw_v,
    q_s, read_s, mix2, wo2, ps, pf, pr, resz, sel, x2, xn, wga, wup, h2, wd2,
    ds, ret, flat, qs, qf, qr,
    ld, ld2,
    p1s, p1r, rls, rlr, wos, wor, wds, wdr, mxs, mxr, p3s, p3r, p4s, p4r,
    p5s, p5r, xls, xlr, hs, hr, p6s, p6r, p7s, p7r,
):
    n_ep = nx * ny
    rows = tokens.shape[0]
    ep = lax.axis_index("ep")
    tp = lax.axis_index("tp")
    z = lax.div(tp, 2)
    c = lax.rem(tp, 2)
    o = 1 - c
    partner = 2 * z + o
    ye = lax.div(ep, nx)
    xe = lax.rem(ep, nx)
    half = nz * 128

    def up_z(d):
        return lax.rem(z + d, nz)

    def down_z(d):
        return lax.rem(z + nz - d, nz)

    def up_ep(d):
        dy, dx = divmod(d, nx)
        return lax.rem(ye + dy, ny) * nx + lax.rem(xe + dx, nx)

    def down_ep(d):
        dy, dx = divmod(d, nx)
        return lax.rem(ye + ny - dy, ny) * nx + lax.rem(xe + nx - dx, nx)

    def hops(d):
        dy, dx = divmod(d, nx)
        return min(dx, nx - dx) + min(dy, ny - dy)

    z_order = near_first(nz)
    ep_order = sorted(range(1, n_ep), key=lambda d: (hops(d), d))

    def remote(src, dst, ss, rs, e, t):
        return pltpu.make_async_remote_copy(
            src_ref=src, dst_ref=dst, send_sem=ss, recv_sem=rs,
            device_id=(e, t), device_id_type=pl.DeviceIdType.MESH,
        )

    sent = []

    def go(copy):
        copy.start()
        sent.append(copy)
        return copy

    def lanes(i):
        return pl.ds(pl.multiple_of(i * 128, 128), 128)

    tok_ld = pltpu.make_async_copy(tokens, tok.at[tp], ld.at[0])
    tok_ld.start()
    barrier = pltpu.get_barrier_semaphore()
    peers = [(ep, partner)] + [(ep, 2 * up_z(d) + c) for d in z_order]
    peers += [(up_ep(d), tp) for d in ep_order]
    flat[...] = jnp.zeros_like(flat)
    xn[...] = jnp.zeros_like(xn)
    for who in peers:
        pl.semaphore_signal(barrier, inc=1, device_id=who, device_id_type=pl.DeviceIdType.MESH)
    rt_block = lanes(lax.div(ep * rows, 128))
    first = [
        (wq, wqk_v.at[0:DK, :]), (wk, wqk_v.at[DK : 2 * DK, :]), (wv, wv_v), (wg, wg_v), (prior, prior_v),
        (decay_in, decay), (norm_in, nin_v), (norm_moe, nmoe_v),
        (routes.at[:, rt_block], rt_v), (route_w.at[:, rt_block], rw_v),
    ]
    first = [pltpu.make_async_copy(a, b, ld.at[i + 1]) for i, (a, b) in enumerate(first)]
    for copy in first:
        copy.start()
    pl.semaphore_wait(barrier, len(peers))
    tok_ld.wait()

    p1 = {}
    for d in z_order:
        p1[d] = go(remote(tok.at[tp], tok.at[tp], p1s.at[d], p1r.at[d], ep, 2 * up_z(d) + c))
    relay = {0: go(remote(tok.at[tp], tok.at[tp], rls.at[0], rlr.at[0], ep, partner))}

    wo_swap = []
    wd_swap = []
    rows_d = edown.shape[0]
    my_wo = pl.ds(pl.multiple_of(c * 128, 128), 128)
    loads = []

    def load(a, b):
        copy = pltpu.make_async_copy(a, b, ld2.at[len(loads)])
        copy.start()
        loads.append(copy)
        return copy

    wo_load = []
    for i in range(nz):
        dst = wo2.at[my_wo, pl.ds(i * 128, 128)]
        wo_load.append(load(wo.at[:, lanes(2 * i + c)], dst))
        wo_swap.append(
            go(remote(wo.at[:, lanes(2 * i + o)], dst, wos.at[i], wor.at[i], ep, partner))
        )
    e_load = []
    for j in range(2 * nz):
        k = (j % 2) * nz + j // 2
        src, dst = pl.ds(j * 128, 128), pl.ds(k * 128, 128)
        e_load.append(load(egate.at[:, src], wga.at[:, dst]))
        e_load.append(load(eup.at[:, src], wup.at[:, dst]))
    d_load = []
    for i in range(nz):
        dst = wd2.at[c, :, pl.ds(i * 128, 128)]
        d_load.append(load(edown.at[:, lanes(2 * i + c)], dst))
        wd_swap.append(
            go(remote(edown.at[:, lanes(2 * i + o)], dst, wds.at[i], wdr.at[i], ep, partner))
        )

    for copy in first:
        copy.wait()

    width = SLOT * n_ep
    side = lax.rem(ep * rows, 128)
    r01 = rt_v[...]
    w01 = rw_v[...]
    r_all, w_all = r01, w01
    for at in range(rows, 128, rows):
        shifted = side == at
        r01 = jnp.where(shifted, jnp.concatenate([r_all[:, at:], r_all[:, :at]], 1), r01)
        w01 = jnp.where(shifted, jnp.concatenate([w_all[:, at:], w_all[:, :at]], 1), w01)
    at = lax.broadcasted_iota(jnp.int32, (width, 128), 0)
    label = at >> 4
    place = (at & (SLOT - 1)).astype(F32)
    m0 = r01[0:1, :] == label
    m1 = r01[1:2, :] == label
    chosen = jnp.where(m0 | m1, 1.0, 0.0)
    before = lax.broadcasted_iota(jnp.int32, (128, 128), 0) < lax.broadcasted_iota(
        jnp.int32, (128, 128), 1
    )
    rank = jnp.dot(
        chosen.astype(BF16), jnp.where(before, 1.0, 0.0).astype(BF16), preferred_element_type=F32
    )
    hit = jnp.where(rank == place, chosen, 0.0)
    picked = hit[:, :rows].astype(BF16)
    weight_t = hit * jnp.where(m0, w01[0:1, :], w01[1:2, :])
    spread = weight_t.T[:rows, :]
    spread_hi = spread.astype(BF16)
    spread_lo = (spread - spread_hi.astype(F32)).astype(BF16)
    spread2 = jnp.concatenate([spread_hi, spread_lo], 0)

    for d in z_order:
        p1[d].wait_recv()
        j = 2 * down_z(d) + c
        relay[d] = go(remote(tok.at[j], tok.at[j], rls.at[d], rlr.at[d], ep, partner))
    for d in [0] + z_order:
        relay[d].wait_recv()

    square = jnp.zeros((rows, 128), F32)
    blocks = [tok[j].astype(F32) for j in range(2 * nz)]
    for block in blocks:
        square += block * block
    factor = lax.rsqrt(jnp.sum(square, -1, keepdims=True) / (2 * half) + EPSILON)
    normed_in = jnp.concatenate(
        [(b * factor * nin_v[j : j + 1, :]).astype(BF16) for j, b in enumerate(blocks)], 1
    )

    def project(weight, across):
        dims = (((1,), (across,)), ((), ()))
        made = lax.dot_general(normed_in, weight[...], dims, preferred_element_type=F32)
        return made.astype(BF16).astype(F32)

    query_key = project(wqk_v, 1)
    query = query_key[:, :DK]
    q_s[...] = query
    keyed = query_key[:, DK:] * DK ** (-0.5)
    valued = project(wv_v, 0)
    gate_pre = project(wg_v, 0)
    k_out[...] = keyed
    v_out[...] = valued

    def group(i, _):
        at8 = pl.ds(pl.multiple_of(i * 8, 8), 8)
        read_s[at8, :] = jnp.sum(prior_v[at8] * q_s[at8, :][:, :, None], 1)
        return 0

    lax.fori_loop(0, rows // 8, group, 0)
    keep = 1.0 - decay[0]
    read = keep * read_s[...] + jnp.sum(query * keyed, -1, keepdims=True) * valued
    centred = read - jnp.mean(read, -1, keepdims=True)
    normed = centred * lax.rsqrt(jnp.mean(centred * centred, -1, keepdims=True) + EPSILON)
    mix2[c] = (gate_pre * jax.nn.sigmoid(gate_pre) * normed).astype(BF16)
    mix = go(remote(mix2.at[c], mix2.at[c], mxs.at[0], mxr.at[0], ep, partner))
    for copy in wo_load:
        copy.wait()
    for copy in wo_swap:
        copy.wait_recv()
    mix.wait_recv()
    mixed = jnp.concatenate([mix2[0], mix2[1]], 1)
    part = jnp.dot(mixed, wo2[...], preferred_element_type=F32)
    for i in range(nz):
        piece = part[:, i * 128 : (i + 1) * 128]
        pf[i] = piece
        ps[i] = piece.astype(BF16)

    p3 = [go(remote(ps.at[up_z(d)], pr.at[d], p3s.at[d], p3r.at[d], ep, 2 * up_z(d) + c)) for d in z_order]
    total = tok[tp].astype(F32) + pf[z]
    for d, copy in zip(z_order, p3):
        copy.wait_recv()
    for d in z_order:
        total += pr[d].astype(F32)
    resid = total.astype(BF16)
    resz[z] = resid
    p4 = [go(remote(resz.at[z], resz.at[z], p4s.at[d], p4r.at[d], ep, 2 * up_z(d) + c)) for d in z_order]
    for copy in p4:
        copy.wait_recv()
    whole = jnp.concatenate([resz[i] for i in range(nz)], 1)
    rows_out = jnp.dot(picked, whole, preferred_element_type=F32).astype(BF16)
    for e in range(n_ep):
        sel[e] = rows_out[e * SLOT : e * SLOT + cap, :]

    p5 = {}
    for d in ep_order:
        e = up_ep(d)
        p5[d] = go(remote(sel.at[e], x2.at[c, d], p5s.at[d], p5r.at[d], e, tp))
    xrelay = {0: go(remote(sel.at[ep], x2.at[c, 0], xls.at[0], xlr.at[0], ep, partner))}
    x2[c, 0] = sel[ep]
    for d in ep_order:
        p5[d].wait_recv()
        mine = x2.at[c, d]
        xrelay[d] = go(remote(mine, mine, xls.at[d], xlr.at[d], ep, partner))
    gains = [nmoe_v[2 * i + s : 2 * i + s + 1, :] for s in range(2) for i in range(nz)]
    gain = jnp.concatenate(gains, 1)
    for d in [0] + ep_order:
        xrelay[d].wait_recv()
        block = jnp.concatenate([x2[0, d], x2[1, d]], 1).astype(F32)
        mean = jnp.sum(block * block, -1, keepdims=True) / (2 * half)
        xn[d * SLOT : d * SLOT + cap, :] = (block * lax.rsqrt(mean + EPSILON) * gain).astype(BF16)

    for copy in e_load:
        copy.wait()
    dims = (((1,), (1,)), ((), ()))
    gate_part = lax.dot_general(xn[...], wga[...], dims, preferred_element_type=F32)
    up_part = lax.dot_general(xn[...], wup[...], dims, preferred_element_type=F32)
    h2[c] = (gate_part * jax.nn.sigmoid(gate_part) * up_part).astype(BF16)
    hid = go(remote(h2.at[c], h2.at[c], hs.at[0], hr.at[0], ep, partner))
    for copy in d_load:
        copy.wait()
    for copy in wd_swap:
        copy.wait_recv()
    hid.wait_recv()
    down = jnp.dot(h2[0], wd2[0], preferred_element_type=F32)
    down += jnp.dot(h2[1], wd2[1], preferred_element_type=F32)
    down = down.astype(BF16)
    for d in range(n_ep):
        ds[d] = down[d * SLOT : d * SLOT + cap, :]

    p6 = {}
    for d in ep_order:
        p6[d] = go(
            remote(ds.at[d], ret.at[ep], p6s.at[d], p6r.at[d], down_ep(d), tp)
        )
    ret[ep] = ds[0]
    for d in ep_order:
        p6[d].wait_recv()
    for e in range(n_ep):
        flat[e * SLOT : e * SLOT + cap, :] = ret[e]
    both = jnp.dot(spread2, flat[...], preferred_element_type=F32)
    weighed = both[:rows, :] + both[rows:, :]
    for i in range(nz):
        piece = weighed[:, i * 128 : (i + 1) * 128]
        qf[i] = piece
        qs[i] = piece.astype(BF16)
    p7 = [go(remote(qs.at[up_z(d)], qr.at[d], p7s.at[d], p7r.at[d], ep, 2 * up_z(d) + c)) for d in z_order]
    total = resz[z].astype(F32) + qf[z]
    for copy in p7:
        copy.wait_recv()
    for d in z_order:
        total += qr[d].astype(F32)
    out[...] = total.astype(BF16)
    for copy in sent:
        copy.wait_send()


def on_device(
    nx, ny, nz,
    tokens, prior_state, decay_rate, norm_in, query_weight, key_weight, value_weight,
    gate_weight, out_weight, norm_moe, routes, route_weight, expert_gate, expert_up, expert_down,
):
    rows = tokens.shape[0]
    n_ep = nx * ny
    width = SLOT * n_ep
    half = nz * 128
    full = 2 * half
    ffe = expert_gate.shape[2]
    cap = (3 * routes.shape[1] * rows + 2 * n_ep - 1) // (2 * n_ep)
    hbm = pl.BlockSpec(memory_space=pl.ANY)
    vmem = pl.BlockSpec(memory_space=pltpu.VMEM)
    scratch = [
        pltpu.SMEM((1,), F32),
        pltpu.VMEM((2 * nz, rows, 128), BF16),
        pltpu.VMEM((2 * DK, full), BF16),
        pltpu.VMEM((full, DV), BF16),
        pltpu.VMEM((full, DV), BF16),
        pltpu.VMEM((rows, DK, DV), F32),
        pltpu.VMEM((2 * nz, 128), F32),
        pltpu.VMEM((2 * nz, 128), F32),
        pltpu.VMEM((2, 128), jnp.int32),
        pltpu.VMEM((2, 128), F32),
        pltpu.VMEM((rows, DK), F32),
        pltpu.VMEM((rows, DV), F32),
        pltpu.VMEM((2, rows, DV), BF16),
        pltpu.VMEM((2 * DV, half), BF16),
        pltpu.VMEM((nz, rows, 128), BF16),
        pltpu.VMEM((nz, rows, 128), F32),
        pltpu.VMEM((nz, rows, 128), BF16),
        pltpu.VMEM((nz, rows, 128), BF16),
        pltpu.VMEM((n_ep, cap, half), BF16),
        pltpu.VMEM((2, n_ep, cap, half), BF16),
        pltpu.VMEM((width, full), BF16),
        pltpu.VMEM((ffe, full), BF16),
        pltpu.VMEM((ffe, full), BF16),
        pltpu.VMEM((2, width, ffe), BF16),
        pltpu.VMEM((2, ffe, half), BF16),
        pltpu.VMEM((n_ep, cap, half), BF16),
        pltpu.VMEM((n_ep, cap, half), BF16),
        pltpu.VMEM((width, half), BF16),
        pltpu.VMEM((nz, rows, 128), BF16),
        pltpu.VMEM((nz, rows, 128), F32),
        pltpu.VMEM((nz, rows, 128), BF16),
        pltpu.SemaphoreType.DMA((11,)),
        pltpu.SemaphoreType.DMA((6 * nz,)),
    ]
    for n in (nz, nz, nz, nz, nz, nz, nz, nz, 1, 1, nz, nz, nz, nz, n_ep, n_ep, n_ep, n_ep, 1, 1, n_ep, n_ep, nz, nz):
        scratch.append(pltpu.SemaphoreType.DMA((n,)))
    next_hidden, keyed, valued = pl.pallas_call(
        functools.partial(layer_kernel, nx, ny, nz, cap),
        out_shape=(
            jax.ShapeDtypeStruct((rows, 128), BF16),
            jax.ShapeDtypeStruct((rows, DK), F32),
            jax.ShapeDtypeStruct((rows, DV), F32),
        ),
        in_specs=[hbm] * 15,
        out_specs=(vmem, vmem, vmem),
        scratch_shapes=scratch,
        compiler_params=pltpu.CompilerParams(
            collective_id=0, has_side_effects=True, vmem_limit_bytes=67043328
        ),
        name="layer",
    )(
        tokens, prior_state.reshape(rows, DK, DV), decay_rate, norm_in.reshape(2 * nz, 128),
        query_weight.T, key_weight.T, value_weight, gate_weight, out_weight,
        norm_moe.reshape(2 * nz, 128), routes.T, route_weight.T,
        expert_gate.reshape(full, ffe).T, expert_up.reshape(full, ffe).T, expert_down.reshape(ffe, full),
    )
    keep = 1.0 - decay_rate[0]
    new_state = keep * prior_state[:, 0] + keyed[:, :, None] * valued[:, None, :]
    return (next_hidden, new_state[:, None])


def solution(mesh):
    n_ep, n_tp = mesh.shape["ep"], mesh.shape["tp"]
    nx = next(i for i in range(1, n_ep + 1) if i * i >= n_ep)
    placed = (
        P("ep", "tp"),
        P("ep", "tp", None, None),
        P("tp"),
        P(),
        P(None, "tp"),
        P(None, "tp"),
        P(None, "tp"),
        P(None, "tp"),
        P("tp", None),
        P(),
        P(),
        P(),
        P("ep", None, "tp"),
        P("ep", None, "tp"),
        P("ep", "tp", None),
    )
    return jax.shard_map(
        functools.partial(on_device, nx, n_ep // nx, n_tp // 2),
        mesh=mesh,
        in_specs=placed,
        out_specs=(P("ep", "tp"), P("ep", "tp", None, None)),
        check_vma=False,
    )
```

```python
import functools
import jax
import jax.numpy as jnp
from jax import lax
from jax.experimental import pallas as pl
from jax.experimental.pallas import tpu as pltpu
from jax.sharding import PartitionSpec as P

DK = 64
DV = 128
SLOT = 16
EPSILON = 1e-06
F32 = jnp.float32
BF16 = jnp.bfloat16


def near_first(n):
    return sorted(range(1, n), key=lambda d: (min(d, n - d), d))


def layer_kernel(
    nx, ny, nz, cap,
    tokens, prior, decay_in, norm_in, wq, wk, wv, wg, wo, norm_moe,
    routes, route_w, egate, eup, edown,
    out, k_out, v_out,
    decay, tok_own, tok, wqk_v, wvg_v, prior_v, nin_v, nmoe_v, rt_v, rw_v, keep2,
    q_s, k_s, v_s, k_in, v_in, read_s, wo2, ps, pr, resz, sel, x2, xn, wga, wup, wd2,
    ds, ret, flat, qs, qr,
    ld, p1s, p1r, wds, wdr, p3s, p3r, p4s, p4r, p5s, p5r, p6s, p6r, p6o, p7s, p7r,
):
    n_ep = nx * ny
    rows = tokens.shape[0]
    ep = lax.axis_index("ep")
    tp = lax.axis_index("tp")
    z = lax.div(tp, 2)
    c = lax.rem(tp, 2)
    o = 1 - c
    partner = 2 * z + o
    ye = lax.div(ep, nx)
    xe = lax.rem(ep, nx)
    half = nz * 128

    def up_z(d):
        return lax.rem(z + d, nz)

    def down_z(d):
        return lax.rem(z + nz - d, nz)

    def up_ep(d):
        dy, dx = divmod(d, nx)
        return lax.rem(ye + dy, ny) * nx + lax.rem(xe + dx, nx)

    def down_ep(d):
        dy, dx = divmod(d, nx)
        return lax.rem(ye + ny - dy, ny) * nx + lax.rem(xe + nx - dx, nx)

    def hops(d):
        dy, dx = divmod(d, nx)
        return min(dx, nx - dx) + min(dy, ny - dy)

    z_order = near_first(nz)
    ep_order = sorted(range(1, n_ep), key=lambda d: (hops(d), d))

    def remote(src, dst, ss, rs, e, t):
        return pltpu.make_async_remote_copy(
            src_ref=src, dst_ref=dst, send_sem=ss, recv_sem=rs,
            device_id=(e, t), device_id_type=pl.DeviceIdType.MESH,
        )

    sent = []

    def go(copy):
        copy.start()
        sent.append(copy)
        return copy

    def lanes(i):
        return pl.ds(pl.multiple_of(i * 128, 128), 128)

    barrier = pltpu.get_barrier_semaphore()
    peers = [(ep, partner)]
    peers += [(ep, 2 * up_z(d) + p) for d in z_order for p in range(2)]
    peers += [(up_ep(d), 2 * z + p) for d in ep_order for p in range(2)]
    for who in peers:
        pl.semaphore_signal(barrier, inc=1, device_id=who, device_id_type=pl.DeviceIdType.MESH)
    loads = []

    def load(a, b):
        copy = pltpu.make_async_copy(a, b, ld.at[len(loads)])
        copy.start()
        loads.append(copy)
        return copy

    swaps = []

    def swap(a, b):
        i = len(swaps)
        swaps.append(go(remote(a, b, wds.at[i], wdr.at[i], ep, partner)))
        return swaps[i]

    def part_of(i, size):
        return pl.ds(pl.multiple_of(i * size, size), size)

    part = rows // 2
    hid_rows = edown.shape[0]
    tok_ld = load(tokens, tok_own)
    rt_block = lanes(lax.div(ep * rows, 128))
    small_ld = [
        load(decay_in, decay), load(norm_in, nin_v), load(norm_moe, nmoe_v),
        load(routes.at[:, rt_block], rt_v), load(route_w.at[:, rt_block], rw_v),
    ]
    mine_ld = [
        load(wq, wqk_v.at[c, 0:DK, :]), load(wk, wqk_v.at[c, DK : 2 * DK, :]),
        load(wv, wvg_v.at[:, lanes(2 * c)]), load(wg, wvg_v.at[:, lanes(2 * c + 1)]),
        load(prior.at[part_of(c, part)], prior_v.at[c]),
    ]
    wo_load = load(wo, wo2.at[part_of(c, 128), :])
    flat[...] = jnp.zeros_like(flat)
    xn[...] = jnp.zeros_like(xn)
    for copy in small_ld:
        copy.wait()
    keep2[c] = jnp.full((8, 128), 1.0 - decay[0], F32)
    pl.semaphore_wait(barrier, len(peers))
    tok_ld.wait()

    tok[tp] = tok_own[part_of(c, part), :]
    p1 = {}
    for d in z_order + [0]:
        for p in range(2):
            src = tok_own.at[p * part : (p + 1) * part, :]
            copy = remote(src, tok.at[tp], p1s.at[d, p], p1r.at[d, c], ep, 2 * up_z(d) + p)
            if d:
                go(copy)
            else:
                pl.when(c != p)(copy.start)
    keep_swap = swap(keep2.at[c], keep2.at[c])
    first_swap = [
        swap(wq, wqk_v.at[c, 0:DK, :]), swap(wk, wqk_v.at[c, DK : 2 * DK, :]),
        swap(wv, wvg_v.at[:, lanes(2 * c)]), swap(wg, wvg_v.at[:, lanes(2 * c + 1)]),
        swap(prior.at[part_of(o, part)], prior_v.at[c]),
    ]
    wo_swap = swap(wo, wo2.at[part_of(c, 128), :])
    mine = part_of(c, hid_rows)
    e_load = [load(a, b.at[mine, :]) for a, b in [(egate, wga), (eup, wup), (edown, wd2)]]
    gate_swap = swap(egate, wga.at[mine, :])
    width = SLOT * n_ep
    side = lax.rem(ep * rows, 128)
    r01 = rt_v[...]
    w01 = rw_v[...]
    r_all, w_all = r01, w01
    for at in range(rows, 128, rows):
        shifted = side == at
        r01 = jnp.where(shifted, jnp.concatenate([r_all[:, at:], r_all[:, :at]], 1), r01)
        w01 = jnp.where(shifted, jnp.concatenate([w_all[:, at:], w_all[:, :at]], 1), w01)
    at = lax.broadcasted_iota(jnp.int32, (width, 128), 0)
    label = at >> 4
    place = (at & (SLOT - 1)).astype(F32)
    m0 = r01[0:1, :] == label
    m1 = r01[1:2, :] == label
    chosen = jnp.where(m0 | m1, 1.0, 0.0)
    before = lax.broadcasted_iota(jnp.int32, (128, 128), 0) < lax.broadcasted_iota(
        jnp.int32, (128, 128), 1
    )
    rank = jnp.dot(
        chosen.astype(BF16), jnp.where(before, 1.0, 0.0).astype(BF16), preferred_element_type=F32
    )
    hit = jnp.where(rank == place, chosen, 0.0)
    picked = hit[:, :rows].astype(BF16)
    weight_t = hit * jnp.where(m0, w01[0:1, :], w01[1:2, :])
    spread = weight_t.T[:rows, :]
    spread_hi = spread.astype(BF16)
    spread_lo = (spread - spread_hi.astype(F32)).astype(BF16)
    spread2 = jnp.concatenate([spread_hi, spread_lo], 0)

    for d in [0] + z_order:
        for p in range(2):
            copy = remote(tok.at[0], tok.at[0], p1s.at[d, p], p1r.at[d, p], ep, partner)
            if d:
                copy.wait_recv()
            else:
                pl.when(c != p)(copy.wait_recv)
    for copy in mine_ld:
        copy.wait()
    keep_swap.wait_recv()
    for copy in first_swap:
        copy.wait_recv()

    square = jnp.zeros((part, 128), F32)
    blocks = [tok[j].astype(F32) for j in range(2 * nz)]
    for block in blocks:
        square += block * block
    factor = lax.rsqrt(jnp.sum(square, -1, keepdims=True) / (2 * half) + EPSILON)
    normed_in = jnp.concatenate(
        [(b * factor * nin_v[j : j + 1, :]).astype(BF16) for j, b in enumerate(blocks)], 1
    )
    dims = (((1,), (1,)), ((), ()))
    qk = lax.dot_general(normed_in, wqk_v[...].reshape(4 * DK, 2 * half), dims, preferred_element_type=F32)
    qk = qk.astype(BF16).astype(F32)
    vg = jnp.dot(normed_in, wvg_v[...], preferred_element_type=F32).astype(BF16).astype(F32)
    for h in range(2):
        q_s[h] = qk[:, 2 * h * DK : (2 * h + 1) * DK]
        k_of = qk[:, (2 * h + 1) * DK : (2 * h + 2) * DK] * DK ** (-0.5)
        v_of = vg[:, 2 * h * DV : (2 * h + 1) * DV]
        k_s[h] = jnp.concatenate([k_of, jnp.zeros_like(k_of)], 1)
        v_s[h] = v_of
    def group(i, _):
        h = lax.div(i, part // 8)
        at8 = pl.ds(pl.multiple_of(lax.rem(i, part // 8) * 8, 8), 8)
        read_s[h, at8, :] = jnp.sum(prior_v[h, at8] * q_s[h, at8, :][:, :, None], 1)
        return 0

    lax.fori_loop(0, 2 * part // 8, group, 0)
    sides = []
    for h in range(2):
        v_of = v_s[h]
        q_k = jnp.sum(q_s[h] * k_s[h][:, :DK], -1, keepdims=True)
        read = keep2[h][0:1, :] * read_s[h] + q_k * v_of
        centred = read - jnp.mean(read, -1, keepdims=True)
        normed = centred * lax.rsqrt(jnp.mean(centred * centred, -1, keepdims=True) + EPSILON)
        gate_pre = vg[:, (2 * h + 1) * DV : (2 * h + 2) * DV]
        sides.append((gate_pre * jax.nn.sigmoid(gate_pre) * normed).astype(BF16))
    mixed = jnp.concatenate(sides, 1)
    wo_load.wait()
    wo_swap.wait_recv()
    made = jnp.dot(mixed, wo2[...], preferred_element_type=F32).astype(BF16)
    for j in range(2 * nz):
        ps[j] = made[:, j * 128 : (j + 1) * 128]

    for d in z_order + [0]:
        for p in range(2):
            at = 2 * up_z(d) + p
            copy = remote(ps.at[at], pr.at[c, d], p3s.at[d, p], p3r.at[d, c], ep, at)
            if d:
                go(copy)
            else:
                pl.when(c != p)(copy.start)
    pr[c, 0] = ps[tp]
    k_swap = swap(k_s.at[o], k_in)
    v_swap = swap(v_s.at[o], v_in)
    up_swap = swap(eup, wup.at[mine, :])
    for d in [0] + z_order:
        for p in range(2):
            copy = remote(pr.at[0, 0], pr.at[0, 0], p3s.at[d, p], p3r.at[d, p], ep, partner)
            if d:
                copy.wait_recv()
            else:
                pl.when(c != p)(copy.wait_recv)
    for p in range(2):
        total = tok_own[p * part : (p + 1) * part, :].astype(F32)
        for d in range(nz):
            total += pr[p, d].astype(F32)
        resz[z, p * part : (p + 1) * part, :] = total.astype(BF16)
    p4 = {}
    for d in z_order:
        p4[d] = go(remote(resz.at[z], resz.at[z], p4s.at[d], p4r.at[d], ep, 2 * up_z(d) + c))
    for t in [0] + z_order:
        if t:
            p4[t].wait_recv()
        at = down_z(t)
        rows_out = jnp.dot(picked, resz[at], preferred_element_type=F32).astype(BF16)
        for e in range(n_ep):
            sel[e, t] = rows_out[e * SLOT : e * SLOT + cap, :]
        for d in ep_order:
            e = up_ep(d)
            remote(
                sel.at[e, t], x2.at[c, d // 2, at], p5s.at[d], p5r.at[c, d // 2], e, 2 * z + d % 2
            ).start()

        @pl.when(c == 1)
        def _():
            remote(sel.at[ep, t], x2.at[1, 0, at], p5s.at[0], p5r.at[1, 0], ep, 2 * z).start()

        @pl.when(c == 0)
        def _():
            x2[0, 0, at] = sel[ep, t]

    down_swap = swap(edown, wd2.at[mine, :])
    k_swap.wait_recv()
    v_swap.wait_recv()
    k_out[part_of(c, part), :] = k_s[c][:, :DK]
    v_out[part_of(c, part), :] = v_s[c]
    k_out[part_of(o, part), :] = k_in[:, :DK]
    v_out[part_of(o, part), :] = v_in[...]
    slots = n_ep // 2

    def slot_copy(cc, s):
        return remote(sel.at[0], x2.at[cc, s], p5s.at[0], p5r.at[cc, s], ep, partner)

    for s in range(slots):

        @pl.when((c == 1) | (s > 0))
        def _():
            slot_copy(0, s).wait_recv()

        slot_copy(1, s).wait_recv()
        pieces = [x2[j % 2, s, j // 2] for j in range(2 * nz)]
        block = jnp.concatenate(pieces, 1).astype(F32)
        mean = jnp.sum(block * block, -1, keepdims=True) / (2 * half)
        gain = jnp.concatenate([nmoe_v[j : j + 1, :] for j in range(2 * nz)], 1)
        xn[s * SLOT : s * SLOT + cap, :] = (block * lax.rsqrt(mean + EPSILON) * gain).astype(BF16)

    for copy in e_load:
        copy.wait()
    for copy in (gate_swap, up_swap, down_swap):
        copy.wait_recv()
    gate_part = lax.dot_general(xn[...], wga[...], dims, preferred_element_type=F32)
    up_part = lax.dot_general(xn[...], wup[...], dims, preferred_element_type=F32)
    hidden = (gate_part * jax.nn.sigmoid(gate_part) * up_part).astype(BF16)
    back_order = z_order[::-1] + [0]
    for t in back_order:
        at = up_z(t)
        cols = pl.ds(pl.multiple_of(at * 256, 256), 256)
        down = jnp.dot(hidden, wd2[:, cols], preferred_element_type=F32).astype(BF16)
        for s in range(slots):
            for p in range(2):
                ds[t, s, p] = down[s * SLOT : s * SLOT + cap, p * 128 : (p + 1) * 128]
        for s in range(slots):
            d = 2 * s + c
            dx, dy = lax.rem(d, nx), lax.div(d, nx)
            src = lax.rem(ye + ny - dy, ny) * nx + lax.rem(xe + nx - dx, nx)
            for p in range(2):
                if s == 0:
                    @pl.when(c == 1)
                    def _():
                        remote(ds.at[t, s, p], ret.at[at, ep], p6s.at[s, p], p6r.at[t], src, 2 * z + p).start()

                    if p == 0:

                        @pl.when(c == 0)
                        def _():
                            ret[at, ep] = ds[t, s, p]

                    else:

                        @pl.when(c == 0)
                        def _():
                            remote(ds.at[t, s, p], ret.at[at, ep], p6s.at[s, p], p6o.at[t], ep, 2 * z + 1).start()

                else:
                    remote(ds.at[t, s, p], ret.at[at, ep], p6s.at[s, p], p6r.at[t], src, 2 * z + p).start()

    p7 = []
    total = resz[z].astype(F32)
    for t in back_order:
        at = up_z(t)
        most = pl.ds(0, n_ep - 1)
        remote(ret.at[at, most], ret.at[at, most], p6s.at[0, 0], p6r.at[t], ep, partner).wait_recv()

        @pl.when(c == 1)
        def _():
            remote(ret.at[at, 0], ret.at[at, 0], p6s.at[0, 0], p6o.at[t], ep, partner).wait_recv()

        for e in range(n_ep):
            flat[e * SLOT : e * SLOT + cap, :] = ret[at, e]
        both = jnp.dot(spread2, flat[...], preferred_element_type=F32)
        weighed = both[:rows, :] + both[rows:, :]
        if t:
            qs[t] = weighed.astype(BF16)
            p7.append(go(remote(qs.at[t], qr.at[t], p7s.at[t], p7r.at[t], ep, 2 * at + c)))
        else:
            total += weighed
    for copy in p7:
        copy.wait_recv()
    for d in z_order:
        total += qr[d].astype(F32)
    out[...] = total.astype(BF16)
    for p in range(2):
        copy = remote(tok.at[0], tok.at[0], p1s.at[0, p], p1r.at[0, p], ep, partner)
        pl.when(c != p)(copy.wait_send)
        copy = remote(pr.at[0, 0], pr.at[0, 0], p3s.at[0, p], p3r.at[0, p], ep, partner)
        pl.when(c != p)(copy.wait_send)
    for d in ep_order:
        remote(sel.at[0], x2.at[0, 0], p5s.at[d], p5r.at[0, 0], ep, partner).wait_send()

    @pl.when(c == 1)
    def _():
        remote(sel.at[0], x2.at[0, 0], p5s.at[0], p5r.at[0, 0], ep, partner).wait_send()

    for s in range(slots):
        for p in range(2):
            done = remote(ds.at[:, s, p], ds.at[:, s, p], p6s.at[s, p], p6r.at[0], ep, partner)
            if s == 0 and p == 0:
                pl.when(c == 1)(done.wait_send)
            else:
                done.wait_send()
    for copy in sent:
        copy.wait_send()


def on_device(
    nx, ny, nz,
    tokens, prior_state, decay_rate, norm_in, query_weight, key_weight, value_weight,
    gate_weight, out_weight, norm_moe, routes, route_weight, expert_gate, expert_up, expert_down,
):
    rows = tokens.shape[0]
    n_ep = nx * ny
    width = SLOT * n_ep
    half = nz * 128
    full = 2 * half
    ffe = expert_gate.shape[2]
    cap = (3 * routes.shape[1] * rows + 2 * n_ep - 1) // (2 * n_ep)
    hbm = pl.BlockSpec(memory_space=pl.ANY)
    vmem = pl.BlockSpec(memory_space=pltpu.VMEM)
    part = rows // 2
    scratch = [
        pltpu.SMEM((1,), F32),
        pltpu.VMEM((rows, 128), BF16),
        pltpu.VMEM((2 * nz, part, 128), BF16),
        pltpu.VMEM((2, 2 * DK, full), BF16),
        pltpu.VMEM((full, 4 * DV), BF16),
        pltpu.VMEM((2, part, DK, DV), F32),
        pltpu.VMEM((2 * nz, 128), F32),
        pltpu.VMEM((2 * nz, 128), F32),
        pltpu.VMEM((2, 128), jnp.int32),
        pltpu.VMEM((2, 128), F32),
        pltpu.VMEM((2, 8, 128), F32),
        pltpu.VMEM((2, part, DK), F32),
        pltpu.VMEM((2, part, 2 * DK), F32),
        pltpu.VMEM((2, part, DV), F32),
        pltpu.VMEM((part, 2 * DK), F32),
        pltpu.VMEM((part, DV), F32),
        pltpu.VMEM((2, part, DV), F32),
        pltpu.VMEM((2 * DV, full), BF16),
        pltpu.VMEM((2 * nz, part, 128), BF16),
        pltpu.VMEM((2, nz, part, 128), BF16),
        pltpu.VMEM((nz, rows, 128), BF16),
        pltpu.VMEM((n_ep, nz, cap, 128), BF16),
        pltpu.VMEM((2, n_ep // 2, nz, cap, 128), BF16),
        pltpu.VMEM((width // 2, full), BF16),
        pltpu.VMEM((2 * ffe, full), BF16),
        pltpu.VMEM((2 * ffe, full), BF16),
        pltpu.VMEM((2 * ffe, full), BF16),
        pltpu.VMEM((nz, n_ep // 2, 2, cap, 128), BF16),
        pltpu.VMEM((nz, n_ep, cap, 128), BF16),
        pltpu.VMEM((width, 128), BF16),
        pltpu.VMEM((nz, rows, 128), BF16),
        pltpu.VMEM((nz, rows, 128), BF16),
    ]
    pairs = (n_ep // 2, 2)
    two = (nz, 2)
    for n in (16, two, two, 16, 16, two, two, nz, nz, n_ep, pairs[::-1], pairs, nz, nz, nz, nz):
        scratch.append(pltpu.SemaphoreType.DMA(n if isinstance(n, tuple) else (n,)))
    next_hidden, keyed, valued = pl.pallas_call(
        functools.partial(layer_kernel, nx, ny, nz, cap),
        out_shape=(
            jax.ShapeDtypeStruct((rows, 128), BF16),
            jax.ShapeDtypeStruct((rows, DK), F32),
            jax.ShapeDtypeStruct((rows, DV), F32),
        ),
        in_specs=[hbm] * 15,
        out_specs=(vmem, vmem, vmem),
        scratch_shapes=scratch,
        compiler_params=pltpu.CompilerParams(
            collective_id=0, has_side_effects=True, vmem_limit_bytes=67043328
        ),
        name="layer",
    )(
        tokens, prior_state.reshape(rows, DK, DV), decay_rate, norm_in.reshape(2 * nz, 128),
        query_weight.T, key_weight.T, value_weight, gate_weight, out_weight,
        norm_moe.reshape(2 * nz, 128), routes.T, route_weight.T,
        expert_gate.reshape(full, ffe).T, expert_up.reshape(full, ffe).T, expert_down.reshape(ffe, full),
    )
    keep = 1.0 - decay_rate[0]
    new_state = keep * prior_state[:, 0] + keyed[:, :, None] * valued[:, None, :]
    return (next_hidden, new_state[:, None])


def solution(mesh):
    n_ep, n_tp = mesh.shape["ep"], mesh.shape["tp"]
    nx = next(i for i in range(1, n_ep + 1) if i * i >= n_ep)
    placed = (
        P("ep", "tp"),
        P("ep", "tp", None, None),
        P("tp"),
        P(),
        P(None, "tp"),
        P(None, "tp"),
        P(None, "tp"),
        P(None, "tp"),
        P("tp", None),
        P(),
        P(),
        P(),
        P("ep", None, "tp"),
        P("ep", None, "tp"),
        P("ep", "tp", None),
    )
    return jax.shard_map(
        functools.partial(on_device, nx, n_ep // nx, n_tp // 2),
        mesh=mesh,
        in_specs=placed,
        out_specs=(P("ep", "tp"), P("ep", "tp", None, None)),
        check_vma=False,
    )
```

```python
import functools
import jax
import jax.numpy as jnp
from jax import lax
from jax.experimental import pallas as pl
from jax.experimental.pallas import tpu as pltpu
from jax.sharding import PartitionSpec as P

DK = 64
DV = 128
SLOT = 16
CUTS = tuple(range(9))
BACK_CUTS = tuple(range(9))
EPSILON = 1e-06
F32 = jnp.float32
BF16 = jnp.bfloat16


def near_first(n):
    return sorted(range(1, n), key=lambda d: (min(d, n - d), d))


def layer_kernel(
    nx, ny, nz, cap,
    tokens, prior, decay_in, norm_in, wq, wk, wv, wg, wo, norm_moe,
    routes, route_w, egate, eup, edown,
    out, k_out, v_out,
    decay, tok_own, tok, wqk_v, wvg_v, prior_v, nin_v, nmoe_v, rt_v, rw_v, keep2,
    halves, q_s, k_s, v_s, k_in, v_in, k_all, wo2, ps, pr, resz, sel, x2, xg, sq, acc, wgu, wd2,
    ds, ret, flat, qs, qr,
    ld, p1s, p1r, wds, wdr, p3s, p3r, p4s, p4r, p5s, p5r, p5o, p6s, p6r, p6o, p7s, p7r,
):
    n_ep = nx * ny
    rows = tokens.shape[0]
    ep = lax.axis_index("ep")
    tp = lax.axis_index("tp")
    z = lax.div(tp, 2)
    c = lax.rem(tp, 2)
    o = 1 - c
    partner = 2 * z + o
    ye = lax.div(ep, nx)
    xe = lax.rem(ep, nx)
    half = nz * 128

    def up_z(d):
        return lax.rem(z + d, nz)

    def down_z(d):
        return lax.rem(z + nz - d, nz)

    def up_ep(d):
        dy, dx = divmod(d, nx)
        return lax.rem(ye + dy, ny) * nx + lax.rem(xe + dx, nx)

    def down_ep(d):
        dy, dx = divmod(d, nx)
        return lax.rem(ye + ny - dy, ny) * nx + lax.rem(xe + nx - dx, nx)

    def hops(d):
        dy, dx = divmod(d, nx)
        return min(dx, nx - dx) + min(dy, ny - dy)

    z_order = near_first(nz)
    ep_order = sorted(range(1, n_ep), key=lambda d: (hops(d), d))

    def remote(src, dst, ss, rs, e, t):
        return pltpu.make_async_remote_copy(
            src_ref=src, dst_ref=dst, send_sem=ss, recv_sem=rs,
            device_id=(e, t), device_id_type=pl.DeviceIdType.MESH,
        )

    sent = []

    def go(copy):
        copy.start()
        sent.append(copy)
        return copy

    def lanes(i):
        return pl.ds(pl.multiple_of(i * 128, 128), 128)

    barrier = pltpu.get_barrier_semaphore()
    slots = n_ep // 2

    def served(s):
        d = 2 * s + c
        dx, dy = lax.rem(d, nx), lax.div(d, nx)
        return lax.rem(ye + ny - dy, ny) * nx + lax.rem(xe + nx - dx, nx)

    def hello(e, t):
        pl.semaphore_signal(barrier, inc=1, device_id=(e, t), device_id_type=pl.DeviceIdType.MESH)

    for p in range(2):
        for d in z_order:
            hello(ep, 2 * up_z(d) + p)
        for s in range(1, slots):
            hello(served(s), 2 * z + p)
        pl.when(c == 1)(functools.partial(hello, served(0), 2 * z + p))
    hello(ep, partner)
    loads = []

    def load(a, b):
        copy = pltpu.make_async_copy(a, b, ld.at[len(loads)])
        copy.start()
        loads.append(copy)
        return copy

    swaps = []

    def swap(a, b):
        i = len(swaps)
        swaps.append(go(remote(a, b, wds.at[i], wdr.at[i], ep, partner)))
        return swaps[i]

    def part_of(i, size):
        return pl.ds(pl.multiple_of(i * size, size), size)

    part = rows // 2
    hid_rows = edown.shape[0]
    tok_ld = load(tokens, tok_own)
    rt_block = lanes(lax.div(ep * rows, 128))
    small_ld = [
        load(decay_in, decay), load(norm_in, nin_v), load(norm_moe, nmoe_v),
        load(routes.at[:, rt_block], rt_v), load(route_w.at[:, rt_block], rw_v),
    ]
    prior_ld = load(prior.at[part_of(c, part)], prior_v.at[c])
    mine_ld = [
        load(wq, wqk_v.at[c, 0:DK, :]), load(wk, wqk_v.at[c, DK : 2 * DK, :]),
        load(wv, wvg_v.at[:, lanes(2 * c)]), load(wg, wvg_v.at[:, lanes(2 * c + 1)]),
    ]
    wo_load = load(wo, wo2.at[part_of(c, 128), :])
    flat[...] = jnp.zeros_like(flat)
    xg[...] = jnp.zeros_like(xg)
    sq[...] = jnp.zeros_like(sq)
    for copy in small_ld:
        copy.wait()
    keep2[c] = jnp.full((8, 128), 1.0 - decay[0], F32)
    pl.semaphore_wait(barrier, 2 * (nz - 1) + n_ep)
    tok_ld.wait()

    tok[tp] = tok_own[part_of(c, part), :]
    p1 = {}
    for d in z_order[::-1] + [0]:
        for p in range(2):
            src = tok_own.at[p * part : (p + 1) * part, :]
            copy = remote(src, tok.at[tp], p1s.at[d, p], p1r.at[d, c], ep, 2 * up_z(d) + p)
            if d:
                go(copy)
            else:
                pl.when(c != p)(copy.start)
    keep_swap = swap(keep2.at[c], keep2.at[c])
    first_swap = [
        swap(wq, wqk_v.at[c, 0:DK, :]), swap(wk, wqk_v.at[c, DK : 2 * DK, :]),
        swap(wv, wvg_v.at[:, lanes(2 * c)]), swap(wg, wvg_v.at[:, lanes(2 * c + 1)]),
    ]
    prior_swap = swap(prior.at[part_of(o, part)], prior_v.at[c])
    wo_swap = swap(wo, wo2.at[part_of(c, 128), :])
    mine = part_of(c, hid_rows)
    gate_rows = mine
    up_rows = pl.ds(pl.multiple_of((2 + c) * hid_rows, hid_rows), hid_rows)
    e_load = [load(egate, wgu.at[gate_rows, :]), load(eup, wgu.at[up_rows, :]), load(edown, wd2.at[mine, :])]
    gate_swap = swap(egate, wgu.at[gate_rows, :])
    up_swap = swap(eup, wgu.at[up_rows, :])
    width = SLOT * n_ep
    side = lax.rem(ep * rows, 128)
    r01 = rt_v[...]
    w01 = rw_v[...]
    r_all, w_all = r01, w01
    for at in range(rows, 128, rows):
        shifted = side == at
        r01 = jnp.where(shifted, jnp.concatenate([r_all[:, at:], r_all[:, :at]], 1), r01)
        w01 = jnp.where(shifted, jnp.concatenate([w_all[:, at:], w_all[:, :at]], 1), w01)
    at = lax.broadcasted_iota(jnp.int32, (width, 128), 0)
    label = at >> 4
    place = (at & (SLOT - 1)).astype(F32)
    m0 = r01[0:1, :] == label
    m1 = r01[1:2, :] == label
    chosen = jnp.where(m0 | m1, 1.0, 0.0)
    before = lax.broadcasted_iota(jnp.int32, (128, 128), 0) < lax.broadcasted_iota(
        jnp.int32, (128, 128), 1
    )
    rank = jnp.dot(
        chosen.astype(BF16), jnp.where(before, 1.0, 0.0).astype(BF16), preferred_element_type=F32
    )
    hit = jnp.where(rank == place, chosen, 0.0)
    picked = hit[:, :rows].astype(BF16)
    weight_t = hit * jnp.where(m0, w01[0:1, :], w01[1:2, :])
    spread = weight_t.T[:rows, :]
    spread_hi = spread.astype(BF16)
    spread_lo = (spread - spread_hi.astype(F32)).astype(BF16)
    spread2 = jnp.concatenate([spread_hi, spread_lo], 0)

    def split(h):
        def some(i, _):
            at4 = pl.ds(i * 4, 4)
            at256 = pl.ds(pl.multiple_of(i * 4 * DK, 4 * DK), 4 * DK)
            value = prior_v[h, at4].reshape(4 * DK, DV)
            high = value.astype(BF16)
            halves[h, at256, 0:DV] = high
            halves[h, at256, DV : 2 * DV] = (value - high.astype(F32)).astype(BF16)
            return 0

        lax.fori_loop(0, part // 4, some, 0)

    prior_ld.wait()
    split(c)
    for copy in mine_ld:
        copy.wait()
    keep_swap.wait_recv()
    for copy in first_swap:
        copy.wait_recv()
    dims = (((1,), (1,)), ((), ()))
    square = jnp.zeros((part, 128), F32)
    qk = jnp.zeros((part, 4 * DK), F32)
    vg = jnp.zeros((part, 4 * DV), F32)
    for d in [0] + z_order:
        for p in range(2):
            copy = remote(tok.at[0], tok.at[0], p1s.at[d, p], p1r.at[d, p], ep, partner)
            if d:
                copy.wait_recv()
            else:
                pl.when(c != p)(copy.wait_recv)
        if d == z_order[len(z_order) // 2]:
            prior_swap.wait_recv()
            split(o)
        at = down_z(d)
        pair = pl.ds(pl.multiple_of(at * 256, 256), 256)
        scaled = []
        for p in range(2):
            block = tok[2 * at + p].astype(F32)
            square += block * block
            scaled.append((block * nin_v[pl.ds(2 * at + p, 1), :]).astype(BF16))
        scaled = jnp.concatenate(scaled, 1)
        qk += lax.dot_general(scaled, wqk_v[:, :, pair].reshape(4 * DK, 256), dims, preferred_element_type=F32)
        vg += jnp.dot(scaled, wvg_v[pair, :], preferred_element_type=F32)
    factor = lax.rsqrt(jnp.sum(square, -1, keepdims=True) / (2 * half) + EPSILON)
    qk = (qk * factor).astype(BF16)
    vg = (vg * factor).astype(BF16).astype(F32)
    wide = lax.broadcasted_iota(jnp.int32, (part, part * DK), 1)
    own_row = lax.div(wide, DK) == lax.broadcasted_iota(jnp.int32, (part, part * DK), 0)
    reads = []
    for h in range(2):
        query = qk[:, 2 * h * DK : (2 * h + 1) * DK].astype(F32)
        k_of = qk[:, (2 * h + 1) * DK : (2 * h + 2) * DK].astype(F32) * DK ** (-0.5)
        q_s[h] = query
        k_s[h] = jnp.concatenate([k_of, jnp.zeros_like(k_of)], 1)
        v_s[h] = vg[:, 2 * h * DV : (2 * h + 1) * DV]
        double = jnp.concatenate([query, query], 1)
        spread_q = jnp.where(own_row, jnp.concatenate([double] * (part // 2), 1), 0.0).astype(BF16)
        both = jnp.dot(spread_q, halves[h], preferred_element_type=F32)
        reads.append(both[:, :DV] + both[:, DV:])
    sides = []
    for h in range(2):
        v_of = v_s[h]
        q_k = jnp.sum(q_s[h] * k_s[h][:, :DK], -1, keepdims=True)
        read = keep2[h][0:1, :] * reads[h] + q_k * v_of
        centred = read - jnp.mean(read, -1, keepdims=True)
        normed = centred * lax.rsqrt(jnp.mean(centred * centred, -1, keepdims=True) + EPSILON)
        gate_pre = vg[:, (2 * h + 1) * DV : (2 * h + 2) * DV]
        sides.append((gate_pre * jax.nn.sigmoid(gate_pre) * normed).astype(BF16))
    mixed = jnp.concatenate(sides, 1)
    wo_load.wait()
    wo_swap.wait_recv()
    made = jnp.dot(mixed, wo2[...], preferred_element_type=F32).astype(BF16)
    for j in range(2 * nz):
        ps[j] = made[:, j * 128 : (j + 1) * 128]

    for d in z_order[::-1] + [0]:
        for p in range(2):
            at = 2 * up_z(d) + p
            copy = remote(ps.at[at], pr.at[c, d], p3s.at[d, p], p3r.at[d, c], ep, at)
            if d:
                go(copy)
            else:
                pl.when(c != p)(copy.start)
    pr[c, 0] = ps[tp]
    k_swap = swap(k_s.at[o], k_in)
    v_swap = swap(v_s.at[o], v_in)
    down_swap = swap(edown, wd2.at[mine, :])
    k_swap.wait_recv()
    v_swap.wait_recv()
    k_all[part_of(c, part), :] = k_s[c]
    k_all[part_of(o, part), :] = k_in[...]
    k_out[...] = k_all[...].T[:DK, :]
    v_out[part_of(c, part), :] = v_s[c]
    v_out[part_of(o, part), :] = v_in[...]
    for d in [0] + z_order:
        for p in range(2):
            copy = remote(pr.at[0, 0], pr.at[0, 0], p3s.at[d, p], p3r.at[d, p], ep, partner)
            if d:
                copy.wait_recv()
            else:
                pl.when(c != p)(copy.wait_recv)
    for p in range(2):
        total = tok_own[p * part : (p + 1) * part, :].astype(F32)
        for d in range(nz):
            total += pr[p, d].astype(F32)
        resz[z, p * part : (p + 1) * part, :] = total.astype(BF16)
    p4 = {}
    for d in z_order:
        p4[d] = go(remote(resz.at[z], resz.at[z], p4s.at[d], p4r.at[d], ep, 2 * up_z(d) + c))
    order = [0] + z_order
    cuts = sorted({min(i, nz) for i in CUTS})
    for g in range(len(cuts) - 1):
        for i in range(cuts[g], cuts[g + 1]):
            if i:
                p4[order[i]].wait_recv()
            rows_out = jnp.dot(picked, resz[down_z(order[i])], preferred_element_type=F32).astype(BF16)
            for e in range(n_ep):
                sel[e, i] = rows_out[e * SLOT : e * SLOT + cap, :]
        span = slice(cuts[g], cuts[g + 1])
        for d in ep_order:
            e = up_ep(d)
            came = p5r.at[g] if d > 1 else p5o.at[g, c]
            remote(sel.at[e, span], x2.at[c, d // 2, span], p5s.at[d], came, e, 2 * z + d % 2).start()

        @pl.when(c == 1)
        def _():
            remote(sel.at[ep, span], x2.at[1, 0, span], p5s.at[0], p5o.at[g, 1], ep, 2 * z).start()

        @pl.when(c == 0)
        def _():
            x2[0, 0, span] = sel[ep, span]

    for copy in e_load[:2]:
        copy.wait()
    gate_swap.wait_recv()
    up_swap.wait_recv()
    for i in range(nz):
        if i in cuts:
            g = cuts.index(i)
            span = slice(cuts[g], cuts[g + 1])
            most = x2.at[:, 1:slots, span]
            remote(most, most, p5s.at[0], p5r.at[g], ep, partner).wait_recv()
            first = [
                remote(x2.at[p, 0, span], x2.at[p, 0, span], p5s.at[0], p5o.at[g, p], ep, partner)
                for p in range(2)
            ]
            pl.when(c == 1)(first[0].wait_recv)
            first[1].wait_recv()
        at = down_z(order[i])
        gains = [nmoe_v[pl.ds(2 * at + p, 1), :] for p in range(2)]
        for s in range(slots):
            span = slice(s * SLOT, s * SLOT + cap)
            both = [x2[p, s, i].astype(F32) for p in range(2)]
            sq[span, :] += both[0] * both[0] + both[1] * both[1]
            for p in range(2):
                xg[span, p * 128 : (p + 1) * 128] = (both[p] * gains[p]).astype(BF16)
        pair = pl.ds(pl.multiple_of(at * 256, 256), 256)
        more = lax.dot_general(xg[...], wgu[:, pair], dims, preferred_element_type=F32)
        if i:
            acc[...] += more
        else:
            acc[...] = more
    scale = lax.rsqrt(jnp.sum(sq[...], -1, keepdims=True) / (2 * half) + EPSILON)
    gate_part = acc[:, : 2 * hid_rows] * scale
    up_part = acc[:, 2 * hid_rows :] * scale
    hidden = (gate_part * jax.nn.sigmoid(gate_part) * up_part).astype(BF16)
    e_load[2].wait()
    down_swap.wait_recv()
    back = z_order[::-1] + [0]
    backs = sorted({min(i, nz) for i in BACK_CUTS})
    far_slots = sorted(range(slots), key=lambda s: (-max(hops(2 * s), hops(2 * s + 1)), s))
    for g in range(len(backs) - 1):
        for i in range(backs[g], backs[g + 1]):
            cols = pl.ds(pl.multiple_of(up_z(back[i]) * 256, 256), 256)
            down = jnp.dot(hidden, wd2[:, cols], preferred_element_type=F32).astype(BF16)
            for s in range(slots):
                for p in range(2):
                    ds[s, p, i] = down[s * SLOT : s * SLOT + cap, p * 128 : (p + 1) * 128]
        span = slice(backs[g], backs[g + 1])
        for s in far_slots:
            for p in range(2):
                home = remote(
                    ds.at[s, p, span], ret.at[ep, span], p6s.at[s, p], p6r.at[g], served(s), 2 * z + p
                )
                if s:
                    home.start()
                    continue
                pl.when(c == 1)(home.start)
                if p == 0:

                    @pl.when(c == 0)
                    def _():
                        ret[ep, span] = ds[0, 0, span]

                else:
                    other = remote(
                        ds.at[s, p, span], ret.at[ep, span], p6s.at[s, p], p6o.at[g], ep, 2 * z + 1
                    )
                    pl.when(c == 0)(other.start)

    p7 = []
    total = resz[z].astype(F32)
    for i in range(nz):
        if i in backs:
            g = backs.index(i)
            span = slice(backs[g], backs[g + 1])
            most = ret.at[0 : n_ep - 1, span]
            remote(most, most, p6s.at[0, 0], p6r.at[g], ep, partner).wait_recv()
            last = remote(ret.at[0, span], ret.at[0, span], p6s.at[0, 0], p6o.at[g], ep, partner)
            pl.when(c == 1)(last.wait_recv)
        for e in range(n_ep):
            flat[e * SLOT : e * SLOT + cap, :] = ret[e, i]
        both = jnp.dot(spread2, flat[...], preferred_element_type=F32)
        weighed = both[:rows, :] + both[rows:, :]
        t = back[i]
        if t:
            qs[t] = weighed.astype(BF16)
            p7.append(go(remote(qs.at[t], qr.at[t], p7s.at[t], p7r.at[t], ep, 2 * up_z(t) + c)))
        else:
            total += weighed
    for copy in p7:
        copy.wait_recv()
    for d in z_order:
        total += qr[d].astype(F32)
    out[...] = total.astype(BF16)
    for p in range(2):
        copy = remote(tok.at[0], tok.at[0], p1s.at[0, p], p1r.at[0, p], ep, partner)
        pl.when(c != p)(copy.wait_send)
        copy = remote(pr.at[0, 0], pr.at[0, 0], p3s.at[0, p], p3r.at[0, p], ep, partner)
        pl.when(c != p)(copy.wait_send)
    for d in ep_order:
        remote(sel.at[0], sel.at[0], p5s.at[d], p5r.at[0], ep, partner).wait_send()

    @pl.when(c == 1)
    def _():
        remote(sel.at[0], sel.at[0], p5s.at[0], p5r.at[0], ep, partner).wait_send()

    for s in range(slots):
        for p in range(2):
            done = remote(ds.at[s, p], ds.at[s, p], p6s.at[s, p], p6r.at[0], ep, partner)
            if s == 0 and p == 0:
                pl.when(c == 1)(done.wait_send)
            else:
                done.wait_send()
    for copy in sent:
        copy.wait_send()


def state_kernel(decay_in, hidden_in, keys_in, values_in, prior_in, hidden_out, state_out, decay, hidden, keys, values, state, sems):
    pieces = 8
    size = values.shape[0] // pieces
    spans = [slice(j * size, (j + 1) * size) for j in range(pieces)]
    small = [(decay_in, decay), (keys_in, keys), (values_in, values), (hidden_in, hidden)]
    loads = [pltpu.make_async_copy(a, b, sems.at[i]) for i, (a, b) in enumerate(small)]
    loads += [pltpu.make_async_copy(prior_in.at[p], state.at[p], sems.at[4 + j]) for j, p in enumerate(spans)]
    for copy in loads:
        copy.start()
    for copy in loads[:4]:
        copy.wait()
    stores = [pltpu.make_async_copy(hidden, hidden_out, sems.at[4 + pieces])]
    stores[0].start()
    keep = 1.0 - decay[0]
    for j, p in enumerate(spans):
        loads[4 + j].wait()
        for row in range(p.start, p.stop):
            state[row] = keep * state[row] + keys[:, row : row + 1] * values[row : row + 1, :]
        stores.append(pltpu.make_async_copy(state.at[p], state_out.at[p], sems.at[5 + pieces + j]))
        stores[-1].start()
    for copy in stores:
        copy.wait()


def on_device(
    nx, ny, nz,
    tokens, prior_state, decay_rate, norm_in, query_weight, key_weight, value_weight,
    gate_weight, out_weight, norm_moe, routes, route_weight, expert_gate, expert_up, expert_down,
):
    rows = tokens.shape[0]
    n_ep = nx * ny
    width = SLOT * n_ep
    half = nz * 128
    full = 2 * half
    ffe = expert_gate.shape[2]
    cap = (3 * routes.shape[1] * rows + 2 * n_ep - 1) // (2 * n_ep)
    hbm = pl.BlockSpec(memory_space=pltpu.HBM)
    vmem = pl.BlockSpec(memory_space=pltpu.VMEM)
    part = rows // 2
    scratch = [
        pltpu.SMEM((1,), F32),
        pltpu.VMEM((rows, 128), BF16),
        pltpu.VMEM((2 * nz, part, 128), BF16),
        pltpu.VMEM((2, 2 * DK, full), BF16),
        pltpu.VMEM((full, 4 * DV), BF16),
        pltpu.VMEM((2, part, DK, DV), F32),
        pltpu.VMEM((2 * nz, 128), F32),
        pltpu.VMEM((2 * nz, 128), F32),
        pltpu.VMEM((2, 128), jnp.int32),
        pltpu.VMEM((2, 128), F32),
        pltpu.VMEM((2, 8, 128), F32),
        pltpu.VMEM((2, part * DK, 2 * DV), BF16),
        pltpu.VMEM((2, part, DK), F32),
        pltpu.VMEM((2, part, 2 * DK), F32),
        pltpu.VMEM((2, part, DV), F32),
        pltpu.VMEM((part, 2 * DK), F32),
        pltpu.VMEM((part, DV), F32),
        pltpu.VMEM((rows, 2 * DK), F32),
        pltpu.VMEM((2 * DV, full), BF16),
        pltpu.VMEM((2 * nz, part, 128), BF16),
        pltpu.VMEM((2, nz, part, 128), BF16),
        pltpu.VMEM((nz, rows, 128), BF16),
        pltpu.VMEM((n_ep, nz, cap, 128), BF16),
        pltpu.VMEM((2, n_ep // 2, nz, cap, 128), BF16),
        pltpu.VMEM((width // 2, 256), BF16),
        pltpu.VMEM((width // 2, 128), F32),
        pltpu.VMEM((width // 2, 4 * ffe), F32),
        pltpu.VMEM((4 * ffe, full), BF16),
        pltpu.VMEM((2 * ffe, full), BF16),
        pltpu.VMEM((n_ep // 2, 2, nz, cap, 128), BF16),
        pltpu.VMEM((n_ep, nz, cap, 128), BF16),
        pltpu.VMEM((width, 128), BF16),
        pltpu.VMEM((nz, rows, 128), BF16),
        pltpu.VMEM((nz, rows, 128), BF16),
    ]
    pairs = (n_ep // 2, 2)
    two = (nz, 2)
    for n in (16, two, two, 16, 16, two, two, nz, nz, n_ep, nz, two, pairs, nz, nz, nz, nz):
        scratch.append(pltpu.SemaphoreType.DMA(n if isinstance(n, tuple) else (n,)))
    next_hidden, keyed, valued = pl.pallas_call(
        functools.partial(layer_kernel, nx, ny, nz, cap),
        out_shape=(
            jax.ShapeDtypeStruct((rows, 128), BF16),
            jax.ShapeDtypeStruct((DK, rows), F32),
            jax.ShapeDtypeStruct((rows, DV), F32),
        ),
        in_specs=[hbm] * 15,
        out_specs=(vmem, vmem, vmem),
        scratch_shapes=scratch,
        compiler_params=pltpu.CompilerParams(
            collective_id=0, has_side_effects=True, vmem_limit_bytes=67043328
        ),
        name="layer",
    )(
        tokens, prior_state.reshape(rows, DK, DV), decay_rate, norm_in.reshape(2 * nz, 128),
        query_weight.T, key_weight.T, value_weight, gate_weight, out_weight,
        norm_moe.reshape(2 * nz, 128), routes.T, route_weight.T,
        expert_gate.reshape(full, ffe).T, expert_up.reshape(full, ffe).T, expert_down.reshape(ffe, full),
    )
    next_hidden, new_state = pl.pallas_call(
        state_kernel,
        out_shape=(jax.ShapeDtypeStruct((rows, 128), BF16), jax.ShapeDtypeStruct((rows, DK, DV), F32)),
        in_specs=[hbm] * 5,
        out_specs=(hbm, hbm),
        scratch_shapes=[
            pltpu.SMEM((1,), F32),
            pltpu.VMEM((rows, 128), BF16),
            pltpu.VMEM((DK, rows), F32),
            pltpu.VMEM((rows, DV), F32),
            pltpu.VMEM((rows, DK, DV), F32),
            pltpu.SemaphoreType.DMA((21,)),
        ],
        compiler_params=pltpu.CompilerParams(vmem_limit_bytes=67043328),
        name="state",
    )(decay_rate, next_hidden, keyed, valued, prior_state.reshape(rows, DK, DV))
    return (next_hidden, new_state[:, None])


def solution(mesh):
    n_ep, n_tp = mesh.shape["ep"], mesh.shape["tp"]
    nx = next(i for i in range(1, n_ep + 1) if i * i >= n_ep)
    placed = (
        P("ep", "tp"),
        P("ep", "tp", None, None),
        P("tp"),
        P(),
        P(None, "tp"),
        P(None, "tp"),
        P(None, "tp"),
        P(None, "tp"),
        P("tp", None),
        P(),
        P(),
        P(),
        P("ep", None, "tp"),
        P("ep", None, "tp"),
        P("ep", "tp", None),
    )
    return jax.shard_map(
        functools.partial(on_device, nx, n_ep // nx, n_tp // 2),
        mesh=mesh,
        in_specs=placed,
        out_specs=(P("ep", "tp"), P("ep", "tp", None, None)),
        check_vma=False,
    )
```

```python
import functools
import jax
import jax.numpy as jnp
from jax import lax
from jax.experimental import pallas as pl
from jax.experimental.pallas import tpu as pltpu
from jax.sharding import PartitionSpec as P

DK = 64
DV = 128
SLOT = 16
CUTS = tuple(range(9))
BACK_CUTS = tuple(range(9))
JOINS = tuple(range(1, 9))
EPSILON = 1e-06
F32 = jnp.float32
BF16 = jnp.bfloat16


def near_first(n):
    return sorted(range(1, n), key=lambda d: (min(d, n - d), d))


def layer_kernel(
    nx, ny, nz, cap,
    tokens, prior, decay_in, norm_in, wq, wk, wv, wg, wo, norm_moe,
    routes, route_w, egate, eup, edown,
    out_hbm,
    out,
    decay, tok_own, tok, wqk_v, wvg_v, prior_v, norms, rt_v, rw_v, keep2,
    halves, q_s, k_s, v_s, kv_in, k_all, wo2, ps, pr, resz, sel, x2, xg, sq, acc, wgu, wd2,
    ds, ret, flat, qs, qr,
    ld, p1s, p1r, wds, wdr, p3s, p3r, p4s, p4r, p5s, p5r, p6s, p6r, p7s, p7r,
):
    n_ep = nx * ny
    rows = tokens.shape[0]
    nin_v, nmoe_v = norms.at[0], norms.at[1]
    ep = lax.axis_index("ep")
    tp = lax.axis_index("tp")
    z = lax.div(tp, 2)
    c = lax.rem(tp, 2)
    o = 1 - c
    partner = 2 * z + o
    ye = lax.div(ep, nx)
    xe = lax.rem(ep, nx)
    half = nz * 128

    def up_z(d):
        return lax.rem(z + d, nz)

    def down_z(d):
        return lax.rem(z + nz - d, nz)

    def up_ep(d):
        dy, dx = divmod(d, nx)
        return lax.rem(ye + dy, ny) * nx + lax.rem(xe + dx, nx)

    def down_ep(d):
        dy, dx = divmod(d, nx)
        return lax.rem(ye + ny - dy, ny) * nx + lax.rem(xe + nx - dx, nx)

    def hops(d):
        dy, dx = divmod(d, nx)
        return min(dx, nx - dx) + min(dy, ny - dy)

    z_order = near_first(nz)
    ep_order = sorted(range(1, n_ep), key=lambda d: (hops(d), d))

    def remote(src, dst, ss, rs, e, t):
        return pltpu.make_async_remote_copy(
            src_ref=src, dst_ref=dst, send_sem=ss, recv_sem=rs,
            device_id=(e, t), device_id_type=pl.DeviceIdType.MESH,
        )

    def go(copy):
        copy.start()
        return copy

    def arrived(ref, sem):
        remote(ref, ref, sem, sem, ep, partner).wait_recv()

    def left(ref, sem):
        remote(ref, ref, sem, sem, ep, partner).wait_send()

    def lanes(i):
        return pl.ds(pl.multiple_of(i * 128, 128), 128)

    barrier = pltpu.get_barrier_semaphore()
    slots = n_ep // 2

    def served(s):
        d = 2 * s + c
        dx, dy = lax.rem(d, nx), lax.div(d, nx)
        return lax.rem(ye + ny - dy, ny) * nx + lax.rem(xe + nx - dx, nx)

    def hello(e, t):
        pl.semaphore_signal(barrier, inc=1, device_id=(e, t), device_id_type=pl.DeviceIdType.MESH)

    for p in range(2):
        for d in z_order:
            hello(ep, 2 * up_z(d) + p)
        for s in range(1, slots):
            hello(served(s), 2 * z + p)
        pl.when(c == 1)(functools.partial(hello, served(0), 2 * z + p))
    hello(ep, partner)
    def load(i, a, b):
        return go(pltpu.make_async_copy(a, b, ld.at[i]))

    def loaded(i, ref):
        pltpu.make_async_copy(ref, ref, ld.at[i]).wait()

    def swap(i, j, a, b):
        return go(remote(a, b, wds.at[i], wdr.at[j], ep, partner))

    def part_of(i, size):
        return pl.ds(pl.multiple_of(i * size, size), size)

    part = rows // 2
    hid_rows = edown.shape[0]
    tok_ld = load(0, tokens, tok_own)
    rt_block = lanes(lax.div(ep * rows, 128))
    load(1, decay_in, decay)
    load(2, norm_in, nin_v)
    load(2, norm_moe, nmoe_v)
    load(3, routes.at[:, rt_block], rt_v)
    load(4, route_w.at[:, rt_block], rw_v)
    load(5, prior.at[part_of(c, part)], prior_v.at[c])
    load(6, wq, wqk_v.at[c, 0:DK, :])
    load(6, wk, wqk_v.at[c, DK : 2 * DK, :])
    load(7, wv, wvg_v.at[:, lanes(2 * c)])
    load(7, wg, wvg_v.at[:, lanes(2 * c + 1)])
    load(8, wo, wo2.at[part_of(c, 128), :])
    flat[...] = jnp.zeros_like(flat)
    xg[...] = jnp.zeros_like(xg)
    sq[...] = jnp.zeros_like(sq)
    pl.semaphore_wait(barrier, 2 * (nz - 1) + n_ep)
    tok_ld.wait()

    tok[tp] = tok_own[part_of(c, part), :]
    p1 = {}
    for d in z_order[::-1] + [0]:
        for p in range(2):
            src = tok_own.at[p * part : (p + 1) * part, :]
            copy = remote(src, tok.at[tp], p1s.at[0], p1r.at[d], ep, 2 * up_z(d) + p)
            if d:
                go(copy)
            else:
                pl.when(c != p)(copy.start)
    loaded(1, decay)
    loaded(2, norms)
    loaded(3, rt_v)
    loaded(4, rw_v)
    keep2[c] = jnp.full((8, 128), 1.0 - decay[0], F32)
    swap(0, 0, keep2.at[c], keep2.at[c])
    swap(1, 1, wq, wqk_v.at[c, 0:DK, :])
    swap(1, 1, wk, wqk_v.at[c, DK : 2 * DK, :])
    swap(1, 1, wv, wvg_v.at[:, lanes(2 * c)])
    swap(1, 1, wg, wvg_v.at[:, lanes(2 * c + 1)])
    swap(4, 2, prior.at[part_of(o, part)], prior_v.at[c])
    swap(5, 3, wo, wo2.at[part_of(c, 128), :])
    mine = part_of(c, hid_rows)
    up_rows = part_of(2 + c, hid_rows)
    load(9, egate, wgu.at[mine, :])
    load(9, eup, wgu.at[up_rows, :])
    load(10, edown, wd2.at[mine, :])
    swap(2, 4, egate, wgu.at[mine, :])
    swap(2, 4, eup, wgu.at[up_rows, :])
    width = SLOT * n_ep
    side = lax.rem(ep * rows, 128)
    r01 = rt_v[...]
    w01 = rw_v[...]
    r_all, w_all = r01, w01
    for at in range(rows, 128, rows):
        shifted = side == at
        r01 = jnp.where(shifted, jnp.concatenate([r_all[:, at:], r_all[:, :at]], 1), r01)
        w01 = jnp.where(shifted, jnp.concatenate([w_all[:, at:], w_all[:, :at]], 1), w01)
    at = lax.broadcasted_iota(jnp.int32, (width, 128), 0)
    label = at >> 4
    place = (at & (SLOT - 1)).astype(F32)
    m0 = r01[0:1, :] == label
    m1 = r01[1:2, :] == label
    chosen = jnp.where(m0 | m1, 1.0, 0.0)
    before = lax.broadcasted_iota(jnp.int32, (128, 128), 0) < lax.broadcasted_iota(
        jnp.int32, (128, 128), 1
    )
    rank = jnp.dot(
        chosen.astype(BF16), jnp.where(before, 1.0, 0.0).astype(BF16), preferred_element_type=F32
    )
    hit = jnp.where(rank == place, chosen, 0.0)
    picked = hit[:, :rows].astype(BF16)
    weight_t = hit * jnp.where(m0, w01[0:1, :], w01[1:2, :])
    spread = weight_t.T[:rows, :]
    spread_hi = spread.astype(BF16)
    spread_lo = (spread - spread_hi.astype(F32)).astype(BF16)
    spread2 = jnp.concatenate([spread_hi, spread_lo], 0)

    def split(h):
        def some(i, _):
            at4 = pl.ds(i * 4, 4)
            at256 = pl.ds(pl.multiple_of(i * 4 * DK, 4 * DK), 4 * DK)
            value = prior_v[h, at4].reshape(4 * DK, DV)
            high = value.astype(BF16)
            halves[h, at256, 0:DV] = high
            halves[h, at256, DV : 2 * DV] = (value - high.astype(F32)).astype(BF16)
            return 0

        lax.fori_loop(0, part // 4, some, 0)

    loaded(5, prior_v.at[c])
    split(c)
    loaded(6, wqk_v.at[c])
    loaded(7, wvg_v.at[:, part_of(c, 256)])
    arrived(keep2.at[o], wdr.at[0])
    arrived(wvg_v.at[0 : 3 * half // 2, :], wdr.at[1])
    dims = (((1,), (1,)), ((), ()))
    square = jnp.zeros((part, 128), F32)
    qk = jnp.zeros((part, 4 * DK), F32)
    vg = jnp.zeros((part, 4 * DV), F32)
    order = [0] + z_order
    for first_at in range(0, nz, 2):
        if first_at + 2 >= nz:
            arrived(prior_v.at[o], wdr.at[2])
            split(o)
        scaled, wqk_part, wvg_part = [], [], []
        for d in order[first_at : first_at + 2]:
            arrived(tok.at[0 : 2 if d else 1], p1r.at[d])
            at = down_z(d)
            pair = pl.ds(pl.multiple_of(at * 256, 256), 256)
            for p in range(2):
                block = tok[2 * at + p].astype(F32)
                square += block * block
                scaled.append((block * nin_v[pl.ds(2 * at + p, 1), :]).astype(BF16))
            wqk_part.append(wqk_v[:, :, pair].reshape(4 * DK, 256))
            wvg_part.append(wvg_v[pair, :])
        scaled = jnp.concatenate(scaled, 1)
        qk += lax.dot_general(scaled, jnp.concatenate(wqk_part, 1), dims, preferred_element_type=F32)
        vg += jnp.dot(scaled, jnp.concatenate(wvg_part, 0), preferred_element_type=F32)
    factor = lax.rsqrt(jnp.sum(square, -1, keepdims=True) / (2 * half) + EPSILON)
    qk = (qk * factor).astype(BF16)
    vg = (vg * factor).astype(BF16).astype(F32)
    across = lax.broadcasted_iota(jnp.int32, (part, part * DK), 1)
    own_row = lax.div(across, DK) == lax.broadcasted_iota(jnp.int32, (part, part * DK), 0)
    reads = []
    for h in range(2):
        query = qk[:, 2 * h * DK : (2 * h + 1) * DK].astype(F32)
        k_of = qk[:, (2 * h + 1) * DK : (2 * h + 2) * DK].astype(F32) * DK ** (-0.5)
        q_s[h] = query
        k_s[h] = jnp.concatenate([k_of, jnp.zeros_like(k_of)], 1)
        v_s[h] = vg[:, 2 * h * DV : (2 * h + 1) * DV]
        double = jnp.concatenate([query, query], 1)
        spread_q = jnp.where(own_row, jnp.concatenate([double] * (part // 2), 1), 0.0).astype(BF16)
        both = jnp.dot(spread_q, halves[h], preferred_element_type=F32)
        reads.append(both[:, :DV] + both[:, DV:])
    sides = []
    for h in range(2):
        v_of = v_s[h]
        q_k = jnp.sum(q_s[h] * k_s[h][:, :DK], -1, keepdims=True)
        read = keep2[h][0:1, :] * reads[h] + q_k * v_of
        centred = read - jnp.mean(read, -1, keepdims=True)
        normed = centred * lax.rsqrt(jnp.mean(centred * centred, -1, keepdims=True) + EPSILON)
        gate_pre = vg[:, (2 * h + 1) * DV : (2 * h + 2) * DV]
        sides.append((gate_pre * jax.nn.sigmoid(gate_pre) * normed).astype(BF16))
    mixed = jnp.concatenate(sides, 1)
    loaded(8, wo2.at[part_of(c, 128), :])
    arrived(wo2.at[part_of(o, 128), :], wdr.at[3])
    made = jnp.dot(mixed, wo2[...], preferred_element_type=F32).astype(BF16)
    for j in range(2 * nz):
        ps[j] = made[:, j * 128 : (j + 1) * 128]

    for d in z_order[::-1] + [0]:
        for p in range(2):
            at = 2 * up_z(d) + p
            copy = remote(ps.at[at], pr.at[c, d], p3s.at[0], p3r.at[0], ep, at)
            if d:
                go(copy)
            else:
                pl.when(c != p)(copy.start)
    pr[c, 0] = ps[tp]
    swap(3, 5, k_s.at[o], kv_in.at[0])
    swap(3, 5, v_s.at[o], kv_in.at[1])
    swap(2, 6, edown, wd2.at[mine, :])
    arrived(kv_in, wdr.at[5])
    k_all[part_of(c, part), :] = k_s[c]
    k_all[part_of(o, part), :] = kv_in[0]
    out[:, 256:384] = jnp.concatenate([k_all[...].T[:DK, :], jnp.zeros((DK, 128 - rows), F32)], 1)
    out[part_of(c, part), 128:256] = v_s[c]
    out[part_of(o, part), 128:256] = kv_in[1]
    arrived(ps.at[0 : 2 * nz - 1], p3r.at[0])
    for p in range(2):
        total = tok_own[p * part : (p + 1) * part, :].astype(F32)
        for d in range(nz):
            total += pr[p, d].astype(F32)
        resz[z, p * part : (p + 1) * part, :] = total.astype(BF16)
    p4 = {}
    for d in z_order:
        p4[d] = go(remote(resz.at[z], resz.at[z], p4s.at[0], p4r.at[d], ep, 2 * up_z(d) + c))
    cuts = sorted({min(i, nz) for i in CUTS})
    for g in range(len(cuts) - 1):
        for i in range(cuts[g], cuts[g + 1]):
            if i:
                p4[order[i]].wait_recv()
            rows_out = jnp.dot(picked, resz[down_z(order[i])], preferred_element_type=F32).astype(BF16)
            for e in range(n_ep):
                sel[e, i] = rows_out[e * SLOT : e * SLOT + cap, :]
        span = slice(cuts[g], cuts[g + 1])
        for d in ep_order:
            e = up_ep(d)
            remote(
                sel.at[e, span], x2.at[c, d // 2, span], p5s.at[0], p5r.at[g], e, 2 * z + d % 2
            ).start()

        @pl.when(c == 1)
        def _():
            remote(sel.at[ep, span], x2.at[1, 0, span], p5s.at[0], p5r.at[g], ep, 2 * z).start()

        @pl.when(c == 0)
        def _():
            x2[0, 0, span] = sel[ep, span]

    loaded(9, wgu.at[0 : 2 * hid_rows, :])
    arrived(wgu.at[0 : 2 * hid_rows, :], wdr.at[4])
    joins = {min(i, nz) for i in JOINS}
    first_join, wide = True, []
    for i in range(nz):
        if i in cuts:
            g = cuts.index(i)
            span = slice(cuts[g], cuts[g + 1])
            pl.when(c == 1)(functools.partial(arrived, sel.at[:, span], p5r.at[g]))
            pl.when(c == 0)(functools.partial(arrived, sel.at[0 : n_ep - 1, span], p5r.at[g]))
        at = down_z(order[i])
        gains = [nmoe_v[pl.ds(2 * at + p, 1), :] for p in range(2)]
        for s in range(slots):
            span = slice(s * SLOT, s * SLOT + cap)
            both = [x2[p, s, i].astype(F32) for p in range(2)]
            sq[span, :] += both[0] * both[0] + both[1] * both[1]
            for p in range(2):
                lane = (2 * len(wide) + p) * 128
                xg[span, lane : lane + 128] = (both[p] * gains[p]).astype(BF16)
        wide.append(wgu[:, pl.ds(pl.multiple_of(at * 256, 256), 256)])
        if i + 1 in joins:
            used = len(wide) * 256
            more = lax.dot_general(
                xg[:, :used], jnp.concatenate(wide, 1), dims, preferred_element_type=F32
            )
            if first_join:
                acc[...] = more
            else:
                acc[...] += more
            first_join, wide = False, []
    scale = lax.rsqrt(jnp.sum(sq[...], -1, keepdims=True) / (2 * half) + EPSILON)
    gate_part = acc[:, : 2 * hid_rows] * scale
    up_part = acc[:, 2 * hid_rows :] * scale
    hidden = (gate_part * jax.nn.sigmoid(gate_part) * up_part).astype(BF16)
    loaded(10, wd2.at[mine, :])
    arrived(wd2.at[mine, :], wdr.at[6])
    back = z_order[::-1] + [0]
    backs = sorted({min(i, nz) for i in BACK_CUTS})
    far_slots = sorted(range(slots), key=lambda s: (-max(hops(2 * s), hops(2 * s + 1)), s))
    for g in range(len(backs) - 1):
        for i in range(backs[g], backs[g + 1]):
            cols = pl.ds(pl.multiple_of(up_z(back[i]) * 256, 256), 256)
            down = jnp.dot(hidden, wd2[:, cols], preferred_element_type=F32).astype(BF16)
            for s in range(slots):
                for p in range(2):
                    ds[s, p, i] = down[s * SLOT : s * SLOT + cap, p * 128 : (p + 1) * 128]
        span = slice(backs[g], backs[g + 1])
        for s, p in [(s, (p + g) % 2) for s in far_slots[g:] + far_slots[:g] for p in range(2)]:
            if True:
                home = remote(
                    ds.at[s, p, span], ret.at[ep, span], p6s.at[0], p6r.at[g], served(s), 2 * z + p
                )
                if s:
                    home.start()
                    continue
                pl.when(c == 1)(home.start)
                if p == 0:

                    @pl.when(c == 0)
                    def _():
                        ret[ep, span] = ds[0, 0, span]

                else:
                    other = remote(
                        ds.at[s, p, span], ret.at[ep, span], p6s.at[0], p6r.at[g], ep, 2 * z + 1
                    )
                    pl.when(c == 0)(other.start)

    total = resz[z].astype(F32)
    for i in range(nz):
        if i in backs:
            g = backs.index(i)
            span = slice(backs[g], backs[g + 1])
            pl.when(c == 1)(functools.partial(arrived, ret.at[:, span], p6r.at[g]))
            pl.when(c == 0)(functools.partial(arrived, ret.at[0 : n_ep - 1, span], p6r.at[g]))
        for e in range(n_ep):
            flat[e * SLOT : e * SLOT + cap, :] = ret[e, i]
        both = jnp.dot(spread2, flat[...], preferred_element_type=F32)
        weighed = both[:rows, :] + both[rows:, :]
        t = back[i]
        if t:
            qs[t] = weighed.astype(BF16)
            go(remote(qs.at[t], qr.at[t], p7s.at[0], p7r.at[0], ep, 2 * up_z(t) + c))
        else:
            total += weighed
    arrived(qr.at[1:nz], p7r.at[0])
    for d in z_order:
        total += qr[d].astype(F32)
    out[:, :128] = total.astype(BF16).astype(F32)
    load(11, out.at[:, 0:128], out_hbm.at[:, 0:128])
    load(11, out.at[:, 128:384], out_hbm.at[:, 128:384])
    left(ps.at[0 : 2 * nz - 1], p1s.at[0])
    left(ps.at[0 : 2 * nz - 1], p3s.at[0])
    left(resz.at[1:nz], p4s.at[0])
    left(qs.at[1:nz], p7s.at[0])
    left(keep2.at[0], wds.at[0])
    left(wvg_v.at[0 : 3 * half // 2, :], wds.at[1])
    left(prior_v.at[0], wds.at[4])
    left(wo2.at[part_of(c, 128), :], wds.at[5])
    left(wgu.at[0 : 3 * hid_rows, :], wds.at[2])
    left(kv_in, wds.at[3])
    for ref, sem in ((sel, p5s), (ds, p6s)):
        pl.when(c == 1)(functools.partial(left, ref, sem.at[0]))
        pl.when(c == 0)(functools.partial(left, sel.at[0 : n_ep - 1], sem.at[0]))
    loaded(11, out)


def state_kernel(decay, made, prior, hidden_out, state_out, hidden, state, sems):
    pieces = 8
    size = state.shape[0] // pieces
    hidden[...] = made[:, :128].astype(BF16)
    stores = [pltpu.make_async_copy(hidden, hidden_out, sems.at[pieces])]
    stores[0].start()
    keep = 1.0 - decay[0]
    for j in range(pieces):
        for row in range(j * size, (j + 1) * size):
            key, value = made[:, 256 + row : 257 + row], made[row : row + 1, 128:256]
            state[row] = keep * prior[row] + key * value
        span = slice(j * size, (j + 1) * size)
        stores.append(pltpu.make_async_copy(state.at[span], state_out.at[span], sems.at[j]))
        stores[-1].start()
    for copy in stores:
        copy.wait()


def on_device(
    nx, ny, nz,
    tokens, prior_state, decay_rate, norm_in, query_weight, key_weight, value_weight,
    gate_weight, out_weight, norm_moe, routes, route_weight, expert_gate, expert_up, expert_down,
):
    rows = tokens.shape[0]
    n_ep = nx * ny
    width = SLOT * n_ep
    half = nz * 128
    full = 2 * half
    ffe = expert_gate.shape[2]
    cap = (3 * routes.shape[1] * rows + 2 * n_ep - 1) // (2 * n_ep)
    hbm = pl.BlockSpec(memory_space=pltpu.HBM)
    vmem = pl.BlockSpec(memory_space=pltpu.VMEM)
    part = rows // 2
    scratch = [
        pltpu.VMEM((rows, 384), F32),
        pltpu.SMEM((1,), F32),
        pltpu.VMEM((rows, 128), BF16),
        pltpu.VMEM((2 * nz, part, 128), BF16),
        pltpu.VMEM((2, 2 * DK, full), BF16),
        pltpu.VMEM((full, 4 * DV), BF16),
        pltpu.VMEM((2, part, DK, DV), F32),
        pltpu.VMEM((2, 2 * nz, 128), F32),
        pltpu.VMEM((2, 128), jnp.int32),
        pltpu.VMEM((2, 128), F32),
        pltpu.VMEM((2, 8, 128), F32),
        pltpu.VMEM((2, part * DK, 2 * DV), BF16),
        pltpu.VMEM((2, part, DK), F32),
        pltpu.VMEM((2, part, 2 * DK), F32),
        pltpu.VMEM((2, part, DV), F32),
        pltpu.VMEM((2, part, DV), F32),
        pltpu.VMEM((rows, 2 * DK), F32),
        pltpu.VMEM((2 * DV, full), BF16),
        pltpu.VMEM((2 * nz, part, 128), BF16),
        pltpu.VMEM((2, nz, part, 128), BF16),
        pltpu.VMEM((nz, rows, 128), BF16),
        pltpu.VMEM((n_ep, nz, cap, 128), BF16),
        pltpu.VMEM((2, n_ep // 2, nz, cap, 128), BF16),
        pltpu.VMEM((width // 2, 1024), BF16),
        pltpu.VMEM((width // 2, 128), F32),
        pltpu.VMEM((width // 2, 4 * ffe), F32),
        pltpu.VMEM((4 * ffe, full), BF16),
        pltpu.VMEM((2 * ffe, full), BF16),
        pltpu.VMEM((n_ep // 2, 2, nz, cap, 128), BF16),
        pltpu.VMEM((n_ep, nz, cap, 128), BF16),
        pltpu.VMEM((width, 128), BF16),
        pltpu.VMEM((nz, rows, 128), BF16),
        pltpu.VMEM((nz, rows, 128), BF16),
    ]
    for n in (12, 1, nz, 6, 7, 1, 1, 1, nz, 1, nz, 1, nz, 1, 1):
        scratch.append(pltpu.SemaphoreType.DMA((n,)))
    made = pl.pallas_call(
        functools.partial(layer_kernel, nx, ny, nz, cap),
        out_shape=jax.ShapeDtypeStruct((rows, 384), F32),
        in_specs=[hbm] * 15,
        out_specs=hbm,
        scratch_shapes=scratch,
        compiler_params=pltpu.CompilerParams(
            collective_id=0, has_side_effects=True, vmem_limit_bytes=64000000
        ),
        name="layer",
    )(
        tokens, prior_state.reshape(rows, DK, DV), decay_rate, norm_in.reshape(2 * nz, 128),
        query_weight.T, key_weight.T, value_weight, gate_weight, out_weight,
        norm_moe.reshape(2 * nz, 128), routes.T, route_weight.T,
        expert_gate.reshape(full, ffe).T, expert_up.reshape(full, ffe).T, expert_down.reshape(ffe, full),
    )
    next_hidden, new_state = pl.pallas_call(
        state_kernel,
        out_shape=(jax.ShapeDtypeStruct((rows, 128), BF16), jax.ShapeDtypeStruct((rows, DK, DV), F32)),
        in_specs=[pl.BlockSpec(memory_space=pltpu.SMEM), vmem, vmem],
        out_specs=(hbm, hbm),
        scratch_shapes=[
            pltpu.VMEM((rows, 128), BF16),
            pltpu.VMEM((rows, DK, DV), F32),
            pltpu.SemaphoreType.DMA((9,)),
        ],
        compiler_params=pltpu.CompilerParams(vmem_limit_bytes=16 * 1024 * 1024),
        name="state",
    )(decay_rate, made, prior_state.reshape(rows, DK, DV))
    return (next_hidden, new_state[:, None])


def solution(mesh):
    n_ep, n_tp = mesh.shape["ep"], mesh.shape["tp"]
    nx = next(i for i in range(1, n_ep + 1) if i * i >= n_ep)
    placed = (
        P("ep", "tp"),
        P("ep", "tp", None, None),
        P("tp"),
        P(),
        P(None, "tp"),
        P(None, "tp"),
        P(None, "tp"),
        P(None, "tp"),
        P("tp", None),
        P(),
        P(),
        P(),
        P("ep", None, "tp"),
        P("ep", None, "tp"),
        P("ep", "tp", None),
    )
    return jax.shard_map(
        functools.partial(on_device, nx, n_ep // nx, n_tp // 2),
        mesh=mesh,
        in_specs=placed,
        out_specs=(P("ep", "tp"), P("ep", "tp", None, None)),
        check_vma=False,
    )
```

```python
import functools
import jax
import jax.numpy as jnp
from jax import lax
from jax.experimental import pallas as pl
from jax.experimental.pallas import tpu as pltpu
from jax.sharding import PartitionSpec as P

DK = 64
DV = 128
SLOT = 16
CUTS = tuple(range(9))
BACK_CUTS = tuple(range(9))
JOINS = tuple(range(1, 9))
EPSILON = 1e-06
F32 = jnp.float32
BF16 = jnp.bfloat16


def near_first(n):
    return sorted(range(1, n), key=lambda d: (min(d, n - d), d))


def layer_kernel(
    nx, ny, nz, cap,
    tokens, prior, decay_in, norm_in, wq, wk, wv, wg, wo, norm_moe,
    routes, route_w, egate, eup, edown,
    out_hbm,
    out,
    decay, tok_own, tok, wqk_v, wvg_v, prior_v, norms, rt_v, rw_v, keep2,
    halves, q_s, k_s, v_s, kv_in, k_all, wo2, ps, pr, resz, sel, x2, xg, sq, acc, wgu, wd2,
    ds, ret, flat, qs, qr,
    ld, p1s, p1r, wds, wdr, p3s, p3r, p4s, p5s, p5r, p6s, p7s,
):
    n_ep = nx * ny
    rows = tokens.shape[0]
    nin_v, nmoe_v = norms.at[0], norms.at[1]
    p4r, p6r, p7r = p1r, p1r, p3r
    ep = lax.axis_index("ep")
    tp = lax.axis_index("tp")
    z = lax.div(tp, 2)
    c = lax.rem(tp, 2)
    o = 1 - c
    partner = 2 * z + o
    ye = lax.div(ep, nx)
    xe = lax.rem(ep, nx)
    half = nz * 128

    def up_z(d):
        return lax.rem(z + d, nz)

    def down_z(d):
        return lax.rem(z + nz - d, nz)

    def up_ep(d):
        dy, dx = divmod(d, nx)
        return lax.rem(ye + dy, ny) * nx + lax.rem(xe + dx, nx)

    def down_ep(d):
        dy, dx = divmod(d, nx)
        return lax.rem(ye + ny - dy, ny) * nx + lax.rem(xe + nx - dx, nx)

    def hops(d):
        dy, dx = divmod(d, nx)
        return min(dx, nx - dx) + min(dy, ny - dy)

    z_order = near_first(nz)
    ep_order = sorted(range(1, n_ep), key=lambda d: (hops(d), d))

    def remote(src, dst, ss, rs, e, t):
        return pltpu.make_async_remote_copy(
            src_ref=src, dst_ref=dst, send_sem=ss, recv_sem=rs,
            device_id=(e, t), device_id_type=pl.DeviceIdType.MESH,
        )

    def go(copy):
        copy.start()
        return copy

    def arrived(ref, sem):
        remote(ref, ref, sem, sem, ep, partner).wait_recv()

    def left(ref, sem):
        remote(ref, ref, sem, sem, ep, partner).wait_send()

    def lanes(i):
        return pl.ds(pl.multiple_of(i * 128, 128), 128)

    barrier = pltpu.get_barrier_semaphore()
    slots = n_ep // 2

    def served(s):
        d = 2 * s + c
        dx, dy = lax.rem(d, nx), lax.div(d, nx)
        return lax.rem(ye + ny - dy, ny) * nx + lax.rem(xe + nx - dx, nx)

    def hello(e, t):
        pl.semaphore_signal(barrier, inc=1, device_id=(e, t), device_id_type=pl.DeviceIdType.MESH)

    for p in range(2):
        for d in z_order:
            hello(ep, 2 * up_z(d) + p)
        for s in range(1, slots):
            hello(served(s), 2 * z + p)
        pl.when(c == 1)(functools.partial(hello, served(0), 2 * z + p))
    hello(ep, partner)
    def load(i, a, b):
        return go(pltpu.make_async_copy(a, b, ld.at[i]))

    def loaded(i, ref):
        pltpu.make_async_copy(ref, ref, ld.at[i]).wait()

    def swap(i, j, a, b):
        return go(remote(a, b, wds.at[i], wdr.at[j], ep, partner))

    def part_of(i, size):
        return pl.ds(pl.multiple_of(i * size, size), size)

    part = rows // 2
    hid_rows = edown.shape[0]
    tok_ld = load(0, tokens, tok_own)
    rt_block = lanes(lax.div(ep * rows, 128))
    load(1, decay_in, decay)
    load(2, norm_in, nin_v)
    load(2, norm_moe, nmoe_v)
    load(3, routes.at[:, rt_block], rt_v)
    load(4, route_w.at[:, rt_block], rw_v)
    load(5, prior.at[part_of(c, part)], prior_v.at[c])
    load(6, wq, wqk_v.at[c, 0:DK, :])
    load(6, wk, wqk_v.at[c, DK : 2 * DK, :])
    load(7, wv, wvg_v.at[:, lanes(2 * c)])
    load(7, wg, wvg_v.at[:, lanes(2 * c + 1)])
    load(8, wo, wo2.at[part_of(c, 128), :])
    flat[...] = jnp.zeros_like(flat)
    xg[...] = jnp.zeros_like(xg)
    sq[...] = jnp.zeros_like(sq)
    pl.semaphore_wait(barrier, 2 * (nz - 1) + n_ep)
    tok_ld.wait()

    tok[tp] = tok_own[part_of(c, part), :]
    p1 = {}
    for d in z_order[::-1] + [0]:
        for p in range(2):
            src = tok_own.at[p * part : (p + 1) * part, :]
            copy = remote(src, tok.at[tp], p1s.at[0], p1r.at[d], ep, 2 * up_z(d) + p)
            if d:
                go(copy)
            else:
                pl.when(c != p)(copy.start)
    loaded(1, decay)
    loaded(2, norms)
    loaded(3, rt_v)
    loaded(4, rw_v)
    keep2[c] = jnp.full((8, 128), 1.0 - decay[0], F32)
    swap(0, 0, keep2.at[c], keep2.at[c])
    swap(1, 1, wq, wqk_v.at[c, 0:DK, :])
    swap(1, 1, wk, wqk_v.at[c, DK : 2 * DK, :])
    swap(1, 1, wv, wvg_v.at[:, lanes(2 * c)])
    swap(1, 1, wg, wvg_v.at[:, lanes(2 * c + 1)])
    swap(4, 2, prior.at[part_of(o, part)], prior_v.at[c])
    swap(5, 3, wo, wo2.at[part_of(c, 128), :])
    mine = part_of(c, hid_rows)
    up_rows = part_of(2 + c, hid_rows)
    load(9, egate, wgu.at[mine, :])
    load(9, eup, wgu.at[up_rows, :])
    load(10, edown, wd2.at[mine, :])
    swap(2, 4, egate, wgu.at[mine, :])
    swap(2, 4, eup, wgu.at[up_rows, :])
    width = SLOT * n_ep
    side = lax.rem(ep * rows, 128)
    r01 = rt_v[...]
    w01 = rw_v[...]
    r_all, w_all = r01, w01
    for at in range(rows, 128, rows):
        shifted = side == at
        r01 = jnp.where(shifted, jnp.concatenate([r_all[:, at:], r_all[:, :at]], 1), r01)
        w01 = jnp.where(shifted, jnp.concatenate([w_all[:, at:], w_all[:, :at]], 1), w01)
    at = lax.broadcasted_iota(jnp.int32, (width, 128), 0)
    label = at >> 4
    place = (at & (SLOT - 1)).astype(F32)
    m0 = r01[0:1, :] == label
    m1 = r01[1:2, :] == label
    chosen = jnp.where(m0 | m1, 1.0, 0.0)
    before = lax.broadcasted_iota(jnp.int32, (128, 128), 0) < lax.broadcasted_iota(
        jnp.int32, (128, 128), 1
    )
    rank = jnp.dot(
        chosen.astype(BF16), jnp.where(before, 1.0, 0.0).astype(BF16), preferred_element_type=F32
    )
    hit = jnp.where(rank == place, chosen, 0.0)
    picked = hit[:, :rows].astype(BF16)
    weight_t = hit * jnp.where(m0, w01[0:1, :], w01[1:2, :])
    spread = weight_t.T[:rows, :]
    spread_hi = spread.astype(BF16)
    spread_lo = (spread - spread_hi.astype(F32)).astype(BF16)
    spread2 = jnp.concatenate([spread_hi, spread_lo], 0)

    def split(h):
        def some(i, _):
            at4 = pl.ds(i * 4, 4)
            at256 = pl.ds(pl.multiple_of(i * 4 * DK, 4 * DK), 4 * DK)
            value = prior_v[h, at4].reshape(4 * DK, DV)
            high = value.astype(BF16)
            halves[h, at256, 0:DV] = high
            halves[h, at256, DV : 2 * DV] = (value - high.astype(F32)).astype(BF16)
            return 0

        lax.fori_loop(0, part // 4, some, 0)

    loaded(5, prior_v.at[c])
    split(c)
    loaded(6, wqk_v.at[c])
    loaded(7, wvg_v.at[:, part_of(c, 256)])
    arrived(keep2.at[o], wdr.at[0])
    arrived(wvg_v.at[0 : 3 * half // 2, :], wdr.at[1])
    dims = (((1,), (1,)), ((), ()))
    square = jnp.zeros((part, 128), F32)
    qk = jnp.zeros((part, 4 * DK), F32)
    vg = jnp.zeros((part, 4 * DV), F32)
    order = [0] + z_order
    for first_at in range(0, nz, 2):
        if first_at + 2 >= nz:
            arrived(prior_v.at[o], wdr.at[2])
            split(o)
        scaled, wqk_part, wvg_part = [], [], []
        for d in order[first_at : first_at + 2]:
            arrived(tok.at[0 : 2 if d else 1], p1r.at[d])
            at = down_z(d)
            pair = pl.ds(pl.multiple_of(at * 256, 256), 256)
            for p in range(2):
                block = tok[2 * at + p].astype(F32)
                square += block * block
                scaled.append((block * nin_v[pl.ds(2 * at + p, 1), :]).astype(BF16))
            wqk_part.append(wqk_v[:, :, pair].reshape(4 * DK, 256))
            wvg_part.append(wvg_v[pair, :])
        scaled = jnp.concatenate(scaled, 1)
        qk += lax.dot_general(scaled, jnp.concatenate(wqk_part, 1), dims, preferred_element_type=F32)
        vg += jnp.dot(scaled, jnp.concatenate(wvg_part, 0), preferred_element_type=F32)
    factor = lax.rsqrt(jnp.sum(square, -1, keepdims=True) / (2 * half) + EPSILON)
    qk = (qk * factor).astype(BF16)
    vg = (vg * factor).astype(BF16).astype(F32)
    across = lax.broadcasted_iota(jnp.int32, (part, part * DK), 1)
    own_row = lax.div(across, DK) == lax.broadcasted_iota(jnp.int32, (part, part * DK), 0)
    reads = []
    for h in range(2):
        query = qk[:, 2 * h * DK : (2 * h + 1) * DK].astype(F32)
        k_of = qk[:, (2 * h + 1) * DK : (2 * h + 2) * DK].astype(F32) * DK ** (-0.5)
        q_s[h] = query
        k_s[h] = jnp.concatenate([k_of, jnp.zeros_like(k_of)], 1)
        v_s[h] = vg[:, 2 * h * DV : (2 * h + 1) * DV]
        double = jnp.concatenate([query, query], 1)
        spread_q = jnp.where(own_row, jnp.concatenate([double] * (part // 2), 1), 0.0).astype(BF16)
        both = jnp.dot(spread_q, halves[h], preferred_element_type=F32)
        reads.append(both[:, :DV] + both[:, DV:])
    sides = []
    for h in range(2):
        v_of = v_s[h]
        q_k = jnp.sum(q_s[h] * k_s[h][:, :DK], -1, keepdims=True)
        read = keep2[h][0:1, :] * reads[h] + q_k * v_of
        centred = read - jnp.mean(read, -1, keepdims=True)
        normed = centred * lax.rsqrt(jnp.mean(centred * centred, -1, keepdims=True) + EPSILON)
        gate_pre = vg[:, (2 * h + 1) * DV : (2 * h + 2) * DV]
        sides.append((gate_pre * jax.nn.sigmoid(gate_pre) * normed).astype(BF16))
    mixed = jnp.concatenate(sides, 1)
    loaded(8, wo2.at[part_of(c, 128), :])
    arrived(wo2.at[part_of(o, 128), :], wdr.at[3])
    for d in z_order[::-1] + [0]:
        cols = pl.ds(pl.multiple_of(up_z(d) * 256, 256), 256)
        made = jnp.dot(mixed, wo2[:, cols], preferred_element_type=F32).astype(BF16)
        for p in range(2):
            at = 2 * up_z(d) + p
            ps[at] = made[:, p * 128 : (p + 1) * 128]
            copy = remote(ps.at[at], pr.at[c, d], p3s.at[0], p3r.at[0], ep, at)
            if d:
                go(copy)
            else:
                pl.when(c != p)(copy.start)
    pr[c, 0] = ps[tp]
    swap(3, 5, k_s.at[o], kv_in.at[0])
    swap(3, 5, v_s.at[o], kv_in.at[1])
    swap(2, 6, edown, wd2.at[mine, :])
    arrived(kv_in, wdr.at[5])
    k_all[part_of(c, part), :] = k_s[c]
    k_all[part_of(o, part), :] = kv_in[0]
    out[:, 256:384] = jnp.concatenate([k_all[...].T[:DK, :], jnp.zeros((DK, 128 - rows), F32)], 1)
    out[part_of(c, part), 128:256] = v_s[c]
    out[part_of(o, part), 128:256] = kv_in[1]
    arrived(ps.at[0 : 2 * nz - 1], p3r.at[0])
    for p in range(2):
        total = tok_own[p * part : (p + 1) * part, :].astype(F32)
        for d in range(nz):
            total += pr[p, d].astype(F32)
        resz[z, p * part : (p + 1) * part, :] = total.astype(BF16)
    p4 = {}
    for d in z_order:
        p4[d] = go(remote(resz.at[z], resz.at[z], p4s.at[0], p4r.at[d], ep, 2 * up_z(d) + c))
    cuts = sorted({min(i, nz) for i in CUTS})
    for g in range(len(cuts) - 1):
        for i in range(cuts[g], cuts[g + 1]):
            if i:
                p4[order[i]].wait_recv()
            rows_out = jnp.dot(picked, resz[down_z(order[i])], preferred_element_type=F32).astype(BF16)
            for e in range(n_ep):
                sel[e, i] = rows_out[e * SLOT : e * SLOT + cap, :]
        span = slice(cuts[g], cuts[g + 1])
        for d in ep_order[::-1]:
            e = up_ep(d)
            remote(
                sel.at[e, span], x2.at[c, d // 2, span], p5s.at[0], p5r.at[g], e, 2 * z + d % 2
            ).start()

        @pl.when(c == 1)
        def _():
            remote(sel.at[ep, span], x2.at[1, 0, span], p5s.at[0], p5r.at[g], ep, 2 * z).start()

        @pl.when(c == 0)
        def _():
            x2[0, 0, span] = sel[ep, span]

    loaded(9, wgu.at[0 : 2 * hid_rows, :])
    arrived(wgu.at[0 : 2 * hid_rows, :], wdr.at[4])
    joins = {min(i, nz) for i in JOINS}
    first_join, wide = True, []
    for i in range(nz):
        if i in cuts:
            g = cuts.index(i)
            span = slice(cuts[g], cuts[g + 1])
            pl.when(c == 1)(functools.partial(arrived, sel.at[:, span], p5r.at[g]))
            pl.when(c == 0)(functools.partial(arrived, sel.at[0 : n_ep - 1, span], p5r.at[g]))
        at = down_z(order[i])
        gains = [nmoe_v[pl.ds(2 * at + p, 1), :] for p in range(2)]
        for s in range(slots):
            span = slice(s * SLOT, s * SLOT + cap)
            both = [x2[p, s, i].astype(F32) for p in range(2)]
            sq[span, :] += both[0] * both[0] + both[1] * both[1]
            for p in range(2):
                lane = (2 * len(wide) + p) * 128
                xg[span, lane : lane + 128] = (both[p] * gains[p]).astype(BF16)
        wide.append(wgu[:, pl.ds(pl.multiple_of(at * 256, 256), 256)])
        if i + 1 in joins:
            used = len(wide) * 256
            more = lax.dot_general(
                xg[:, :used], jnp.concatenate(wide, 1), dims, preferred_element_type=F32
            )
            if first_join:
                acc[...] = more
            elif i + 1 < nz:
                acc[...] += more
            first_join, wide = False, []
    scale = lax.rsqrt(jnp.sum(sq[...], -1, keepdims=True) / (2 * half) + EPSILON)
    gate_part = (acc[:, : 2 * hid_rows] + more[:, : 2 * hid_rows]) * scale
    up_part = (acc[:, 2 * hid_rows :] + more[:, 2 * hid_rows :]) * scale
    hidden = (gate_part * jax.nn.sigmoid(gate_part) * up_part).astype(BF16)
    loaded(10, wd2.at[mine, :])
    arrived(wd2.at[mine, :], wdr.at[6])
    back = z_order[::-1] + [0]
    backs = sorted({min(i, nz) for i in BACK_CUTS})
    far_slots = sorted(range(slots), key=lambda s: (-max(hops(2 * s), hops(2 * s + 1)), s))
    for g in range(len(backs) - 1):
        for i in range(backs[g], backs[g + 1]):
            cols = pl.ds(pl.multiple_of(up_z(back[i]) * 256, 256), 256)
            down = jnp.dot(hidden, wd2[:, cols], preferred_element_type=F32).astype(BF16)
            for s in range(slots):
                for p in range(2):
                    ds[s, p, i] = down[s * SLOT : s * SLOT + cap, p * 128 : (p + 1) * 128]
        span = slice(backs[g], backs[g + 1])
        for s, p in [(s, (p + g) % 2) for s in far_slots[g:] + far_slots[:g] for p in range(2)]:
            if True:
                home = remote(
                    ds.at[s, p, span], ret.at[ep, span], p6s.at[0], p6r.at[g], served(s), 2 * z + p
                )
                if s:
                    home.start()
                    continue
                pl.when(c == 1)(home.start)
                if p == 0:

                    @pl.when(c == 0)
                    def _():
                        ret[ep, span] = ds[0, 0, span]

                else:
                    other = remote(
                        ds.at[s, p, span], ret.at[ep, span], p6s.at[0], p6r.at[g], ep, 2 * z + 1
                    )
                    pl.when(c == 0)(other.start)

    total = resz[z].astype(F32)
    for i in range(nz):
        if i in backs:
            g = backs.index(i)
            span = slice(backs[g], backs[g + 1])
            pl.when(c == 1)(functools.partial(arrived, ret.at[:, span], p6r.at[g]))
            pl.when(c == 0)(functools.partial(arrived, ret.at[0 : n_ep - 1, span], p6r.at[g]))
        for e in range(n_ep):
            flat[e * SLOT : e * SLOT + cap, :] = ret[e, i]
        both = jnp.dot(spread2, flat[...], preferred_element_type=F32)
        weighed = both[:rows, :] + both[rows:, :]
        t = back[i]
        if t:
            qs[t] = weighed.astype(BF16)
            go(remote(qs.at[t], qr.at[t], p7s.at[0], p7r.at[0], ep, 2 * up_z(t) + c))
        else:
            total += weighed
    arrived(qr.at[1:nz], p7r.at[0])
    for d in z_order:
        total += qr[d].astype(F32)
    out[:, :128] = total.astype(BF16).astype(F32)
    load(11, out.at[:, 0:128], out_hbm.at[:, 0:128])
    load(11, out.at[:, 128:384], out_hbm.at[:, 128:384])
    left(ps.at[0 : 2 * nz - 1], p1s.at[0])
    left(ps.at[0 : 2 * nz - 1], p3s.at[0])
    left(resz.at[1:nz], p4s.at[0])
    left(qs.at[1:nz], p7s.at[0])
    left(keep2.at[0], wds.at[0])
    left(wvg_v.at[0 : 3 * half // 2, :], wds.at[1])
    left(prior_v.at[0], wds.at[4])
    left(wo2.at[part_of(c, 128), :], wds.at[5])
    left(wgu.at[0 : 3 * hid_rows, :], wds.at[2])
    left(kv_in, wds.at[3])
    for ref, sem in ((sel, p5s), (ds, p6s)):
        pl.when(c == 1)(functools.partial(left, ref, sem.at[0]))
        pl.when(c == 0)(functools.partial(left, sel.at[0 : n_ep - 1], sem.at[0]))
    loaded(11, out)


def state_kernel(decay, made, prior, hidden_out, state_out, hidden, state, sems):
    pieces = 8
    size = state.shape[0] // pieces
    hidden[...] = made[:, :128].astype(BF16)
    stores = [pltpu.make_async_copy(hidden, hidden_out, sems.at[pieces])]
    stores[0].start()
    keep = 1.0 - decay[0]
    for j in range(pieces):
        for row in range(j * size, (j + 1) * size):
            key, value = made[:, 256 + row : 257 + row], made[row : row + 1, 128:256]
            state[row] = keep * prior[row] + key * value
        span = slice(j * size, (j + 1) * size)
        stores.append(pltpu.make_async_copy(state.at[span], state_out.at[span], sems.at[j]))
        stores[-1].start()
    for copy in stores:
        copy.wait()


def on_device(
    nx, ny, nz,
    tokens, prior_state, decay_rate, norm_in, query_weight, key_weight, value_weight,
    gate_weight, out_weight, norm_moe, routes, route_weight, expert_gate, expert_up, expert_down,
):
    rows = tokens.shape[0]
    n_ep = nx * ny
    width = SLOT * n_ep
    half = nz * 128
    full = 2 * half
    ffe = expert_gate.shape[2]
    cap = (3 * routes.shape[1] * rows + 2 * n_ep - 1) // (2 * n_ep)
    hbm = pl.BlockSpec(memory_space=pltpu.HBM)
    vmem = pl.BlockSpec(memory_space=pltpu.VMEM)
    part = rows // 2
    scratch = [
        pltpu.VMEM((rows, 384), F32),
        pltpu.SMEM((1,), F32),
        pltpu.VMEM((rows, 128), BF16),
        pltpu.VMEM((2 * nz, part, 128), BF16),
        pltpu.VMEM((2, 2 * DK, full), BF16),
        pltpu.VMEM((full, 4 * DV), BF16),
        pltpu.VMEM((2, part, DK, DV), F32),
        pltpu.VMEM((2, 2 * nz, 128), F32),
        pltpu.VMEM((2, 128), jnp.int32),
        pltpu.VMEM((2, 128), F32),
        pltpu.VMEM((2, 8, 128), F32),
        pltpu.VMEM((2, part * DK, 2 * DV), BF16),
        pltpu.VMEM((2, part, DK), F32),
        pltpu.VMEM((2, part, 2 * DK), F32),
        pltpu.VMEM((2, part, DV), F32),
        pltpu.VMEM((2, part, DV), F32),
        pltpu.VMEM((rows, 2 * DK), F32),
        pltpu.VMEM((2 * DV, full), BF16),
        pltpu.VMEM((2 * nz, part, 128), BF16),
        pltpu.VMEM((2, nz, part, 128), BF16),
        pltpu.VMEM((nz, rows, 128), BF16),
        pltpu.VMEM((n_ep, nz, cap, 128), BF16),
        pltpu.VMEM((2, n_ep // 2, nz, cap, 128), BF16),
        pltpu.VMEM((width // 2, 1024), BF16),
        pltpu.VMEM((width // 2, 128), F32),
        pltpu.VMEM((width // 2, 4 * ffe), F32),
        pltpu.VMEM((4 * ffe, full), BF16),
        pltpu.VMEM((2 * ffe, full), BF16),
        pltpu.VMEM((n_ep // 2, 2, nz, cap, 128), BF16),
        pltpu.VMEM((n_ep, nz, cap, 128), BF16),
        pltpu.VMEM((width, 128), BF16),
        pltpu.VMEM((nz, rows, 128), BF16),
        pltpu.VMEM((nz, rows, 128), BF16),
    ]
    for n in (12, 1, nz, 6, 7, 1, 1, 1, 1, nz, 1, 1):
        scratch.append(pltpu.SemaphoreType.DMA((n,)))
    made = pl.pallas_call(
        functools.partial(layer_kernel, nx, ny, nz, cap),
        out_shape=jax.ShapeDtypeStruct((rows, 384), F32),
        in_specs=[hbm] * 15,
        out_specs=hbm,
        scratch_shapes=scratch,
        compiler_params=pltpu.CompilerParams(
            collective_id=0, has_side_effects=True, vmem_limit_bytes=64000000
        ),
        name="layer",
    )(
        tokens, prior_state.reshape(rows, DK, DV), decay_rate, norm_in.reshape(2 * nz, 128),
        query_weight.T, key_weight.T, value_weight, gate_weight, out_weight,
        norm_moe.reshape(2 * nz, 128), routes.T, route_weight.T,
        expert_gate.reshape(full, ffe).T, expert_up.reshape(full, ffe).T, expert_down.reshape(ffe, full),
    )
    next_hidden, new_state = pl.pallas_call(
        state_kernel,
        out_shape=(jax.ShapeDtypeStruct((rows, 128), BF16), jax.ShapeDtypeStruct((rows, DK, DV), F32)),
        in_specs=[pl.BlockSpec(memory_space=pltpu.SMEM), vmem, vmem],
        out_specs=(hbm, hbm),
        scratch_shapes=[
            pltpu.VMEM((rows, 128), BF16),
            pltpu.VMEM((rows, DK, DV), F32),
            pltpu.SemaphoreType.DMA((9,)),
        ],
        compiler_params=pltpu.CompilerParams(vmem_limit_bytes=16 * 1024 * 1024),
        name="state",
    )(decay_rate, made, prior_state.reshape(rows, DK, DV))
    return (next_hidden, new_state[:, None])


def solution(mesh):
    n_ep, n_tp = mesh.shape["ep"], mesh.shape["tp"]
    nx = next(i for i in range(1, n_ep + 1) if i * i >= n_ep)
    placed = (
        P("ep", "tp"),
        P("ep", "tp", None, None),
        P("tp"),
        P(),
        P(None, "tp"),
        P(None, "tp"),
        P(None, "tp"),
        P(None, "tp"),
        P("tp", None),
        P(),
        P(),
        P(),
        P("ep", None, "tp"),
        P("ep", None, "tp"),
        P("ep", "tp", None),
    )
    return jax.shard_map(
        functools.partial(on_device, nx, n_ep // nx, n_tp // 2),
        mesh=mesh,
        in_specs=placed,
        out_specs=(P("ep", "tp"), P("ep", "tp", None, None)),
        check_vma=False,
    )
```

```python
import functools
import jax
import jax.numpy as jnp
from jax import lax
from jax.experimental import pallas as pl
from jax.experimental.pallas import tpu as pltpu
from jax.sharding import PartitionSpec as P

DK = 64
DV = 128
SLOT = 16
CUTS = tuple(range(9))
BACK_CUTS = tuple(range(9))
JOINS = tuple(range(1, 9))
EPSILON = 1e-06
F32 = jnp.float32
BF16 = jnp.bfloat16


def near_first(n):
    return sorted(range(1, n), key=lambda d: (min(d, n - d), d))


def layer_kernel(
    nx, ny, nz, cap,
    tokens, prior, decay_in, norm_in, wq, wk, wv, wg, wo, norm_moe,
    routes, route_w, egate, eup, edown,
    out_hbm,
    out,
    decay, tok_own, tok, wqk_v, wvg_v, prior_v, norms, rt_v, rw_v, keep2,
    halves, q_s, k_s, v_s, kv_in, k_all, wo2, ps, pr, resz, sel, x2, xg, sq, acc, wgu, wd2,
    ds, ret, flat, qs, qr,
    ld, p1s, p1r, wds, wdr, p3s, p3r, p4s, p5s, p5r, p6s, p7s,
):
    n_ep = nx * ny
    rows = tokens.shape[0]
    nin_v, nmoe_v = norms.at[0], norms.at[1]
    p4r, p6r, p7r = p1r, p1r, p3r
    ep = lax.axis_index("ep")
    tp = lax.axis_index("tp")
    z = lax.div(tp, 2)
    c = lax.rem(tp, 2)
    o = 1 - c
    partner = 2 * z + o
    ye = lax.div(ep, nx)
    xe = lax.rem(ep, nx)
    half = nz * 128

    def up_z(d):
        return lax.rem(z + d, nz)

    def down_z(d):
        return lax.rem(z + nz - d, nz)

    def up_ep(d):
        dy, dx = divmod(d, nx)
        return lax.rem(ye + dy, ny) * nx + lax.rem(xe + dx, nx)

    def down_ep(d):
        dy, dx = divmod(d, nx)
        return lax.rem(ye + ny - dy, ny) * nx + lax.rem(xe + nx - dx, nx)

    def hops(d):
        dy, dx = divmod(d, nx)
        return min(dx, nx - dx) + min(dy, ny - dy)

    z_order = near_first(nz)
    ep_order = sorted(range(1, n_ep), key=lambda d: (hops(d), d))

    def remote(src, dst, ss, rs, e, t):
        return pltpu.make_async_remote_copy(
            src_ref=src, dst_ref=dst, send_sem=ss, recv_sem=rs,
            device_id=(e, t), device_id_type=pl.DeviceIdType.MESH,
        )

    def go(copy):
        copy.start()
        return copy

    def arrived(ref, sem):
        remote(ref, ref, sem, sem, ep, partner).wait_recv()

    def left(ref, sem):
        remote(ref, ref, sem, sem, ep, partner).wait_send()

    def lanes(i):
        return pl.ds(pl.multiple_of(i * 128, 128), 128)

    barrier = pltpu.get_barrier_semaphore()
    slots = n_ep // 2

    def served(s):
        d = 2 * s + c
        dx, dy = lax.rem(d, nx), lax.div(d, nx)
        return lax.rem(ye + ny - dy, ny) * nx + lax.rem(xe + nx - dx, nx)

    def hello(e, t):
        pl.semaphore_signal(barrier, inc=1, device_id=(e, t), device_id_type=pl.DeviceIdType.MESH)

    for p in range(2):
        for d in z_order:
            hello(ep, 2 * up_z(d) + p)
        for s in range(1, slots):
            hello(served(s), 2 * z + p)
        pl.when(c == 1)(functools.partial(hello, served(0), 2 * z + p))
    hello(ep, partner)
    def load(i, a, b):
        return go(pltpu.make_async_copy(a, b, ld.at[i]))

    def loaded(i, ref):
        pltpu.make_async_copy(ref, ref, ld.at[i]).wait()

    def swap(i, j, a, b):
        return go(remote(a, b, wds.at[i], wdr.at[j], ep, partner))

    def part_of(i, size):
        return pl.ds(pl.multiple_of(i * size, size), size)

    part = rows // 2
    hid_rows = edown.shape[0]
    tok_ld = load(0, tokens, tok_own)
    rt_block = lanes(lax.div(ep * rows, 128))
    load(1, decay_in, decay)
    load(2, norm_in, nin_v)
    load(2, norm_moe, nmoe_v)
    load(3, routes.at[:, rt_block], rt_v)
    load(4, route_w.at[:, rt_block], rw_v)
    load(5, prior.at[part_of(c, part)], prior_v.at[c])
    load(6, wq, wqk_v.at[c, 0:DK, :])
    load(6, wk, wqk_v.at[c, DK : 2 * DK, :])
    load(7, wv, wvg_v.at[:, lanes(2 * c)])
    load(7, wg, wvg_v.at[:, lanes(2 * c + 1)])
    load(8, wo, wo2.at[part_of(c, 128), :])
    flat[...] = jnp.zeros_like(flat)
    xg[...] = jnp.zeros_like(xg)
    sq[...] = jnp.zeros_like(sq)
    pl.semaphore_wait(barrier, 2 * (nz - 1) + n_ep)
    tok_ld.wait()

    tok[tp] = tok_own[part_of(c, part), :]
    p1 = {}
    for d in z_order[::-1] + [0]:
        for p in range(2):
            src = tok_own.at[p * part : (p + 1) * part, :]
            copy = remote(src, tok.at[tp], p1s.at[0], p1r.at[d], ep, 2 * up_z(d) + p)
            if d:
                go(copy)
            else:
                pl.when(c != p)(copy.start)
    loaded(1, decay)
    loaded(2, norms)
    loaded(3, rt_v)
    loaded(4, rw_v)
    keep2[c] = jnp.full((8, 128), 1.0 - decay[0], F32)
    swap(0, 0, keep2.at[c], keep2.at[c])
    swap(1, 1, wq, wqk_v.at[c, 0:DK, :])
    swap(1, 1, wk, wqk_v.at[c, DK : 2 * DK, :])
    swap(1, 1, wv, wvg_v.at[:, lanes(2 * c)])
    swap(1, 1, wg, wvg_v.at[:, lanes(2 * c + 1)])
    swap(4, 2, prior.at[part_of(o, part)], prior_v.at[c])
    swap(5, 3, wo, wo2.at[part_of(c, 128), :])
    mine = part_of(c, hid_rows)
    up_rows = part_of(2 + c, hid_rows)
    load(9, egate, wgu.at[mine, :])
    load(9, eup, wgu.at[up_rows, :])
    load(10, edown, wd2.at[mine, :])
    swap(2, 4, egate, wgu.at[mine, :])
    swap(2, 4, eup, wgu.at[up_rows, :])
    width = SLOT * n_ep
    side = lax.rem(ep * rows, 128)
    r01 = rt_v[...]
    w01 = rw_v[...]
    r_all, w_all = r01, w01
    for at in range(rows, 128, rows):
        shifted = side == at
        r01 = jnp.where(shifted, jnp.concatenate([r_all[:, at:], r_all[:, :at]], 1), r01)
        w01 = jnp.where(shifted, jnp.concatenate([w_all[:, at:], w_all[:, :at]], 1), w01)
    at = lax.broadcasted_iota(jnp.int32, (width, 128), 0)
    label = at >> 4
    place = (at & (SLOT - 1)).astype(F32)
    m0 = r01[0:1, :] == label
    m1 = r01[1:2, :] == label
    chosen = jnp.where(m0 | m1, 1.0, 0.0)
    before = lax.broadcasted_iota(jnp.int32, (128, 128), 0) < lax.broadcasted_iota(
        jnp.int32, (128, 128), 1
    )
    rank = jnp.dot(
        chosen.astype(BF16), jnp.where(before, 1.0, 0.0).astype(BF16), preferred_element_type=F32
    )
    hit = jnp.where(rank == place, chosen, 0.0)
    picked = hit[:, :rows].astype(BF16)
    weight_t = hit * jnp.where(m0, w01[0:1, :], w01[1:2, :])
    spread = weight_t.T[:rows, :]
    spread_hi = spread.astype(BF16)
    spread_lo = (spread - spread_hi.astype(F32)).astype(BF16)
    spread2 = jnp.concatenate([spread_hi, spread_lo], 0)

    def split(h):
        def some(i, _):
            at4 = pl.ds(i * 4, 4)
            at256 = pl.ds(pl.multiple_of(i * 4 * DK, 4 * DK), 4 * DK)
            value = prior_v[h, at4].reshape(4 * DK, DV)
            high = value.astype(BF16)
            halves[h, at256, 0:DV] = high
            halves[h, at256, DV : 2 * DV] = (value - high.astype(F32)).astype(BF16)
            return 0

        lax.fori_loop(0, part // 4, some, 0)

    loaded(5, prior_v.at[c])
    split(c)
    loaded(6, wqk_v.at[c])
    loaded(7, wvg_v.at[:, part_of(c, 256)])
    arrived(keep2.at[o], wdr.at[0])
    arrived(wvg_v.at[0 : 3 * half // 2, :], wdr.at[1])
    dims = (((1,), (1,)), ((), ()))
    square = jnp.zeros((part, 128), F32)
    qk = jnp.zeros((part, 4 * DK), F32)
    vg = jnp.zeros((part, 4 * DV), F32)
    order = [0] + z_order
    for first_at in range(0, nz, 2):
        if first_at + 2 >= nz:
            arrived(prior_v.at[o], wdr.at[2])
            split(o)
        scaled, wqk_part, wvg_part = [], [], []
        for d in order[first_at : first_at + 2]:
            arrived(tok.at[0 : 2 if d else 1], p1r.at[d])
            at = down_z(d)
            pair = pl.ds(pl.multiple_of(at * 256, 256), 256)
            for p in range(2):
                block = tok[2 * at + p].astype(F32)
                square += block * block
                scaled.append((block * nin_v[pl.ds(2 * at + p, 1), :]).astype(BF16))
            wqk_part.append(wqk_v[:, :, pair].reshape(4 * DK, 256))
            wvg_part.append(wvg_v[pair, :])
        scaled = jnp.concatenate(scaled, 1)
        qk += lax.dot_general(scaled, jnp.concatenate(wqk_part, 1), dims, preferred_element_type=F32)
        vg += jnp.dot(scaled, jnp.concatenate(wvg_part, 0), preferred_element_type=F32)
    factor = lax.rsqrt(jnp.sum(square, -1, keepdims=True) / (2 * half) + EPSILON)
    qk = (qk * factor).astype(BF16)
    vg = (vg * factor).astype(BF16).astype(F32)
    across = lax.broadcasted_iota(jnp.int32, (part, part * DK), 1)
    own_row = lax.div(across, DK) == lax.broadcasted_iota(jnp.int32, (part, part * DK), 0)
    reads = []
    for h in range(2):
        query = qk[:, 2 * h * DK : (2 * h + 1) * DK].astype(F32)
        k_of = qk[:, (2 * h + 1) * DK : (2 * h + 2) * DK].astype(F32) * DK ** (-0.5)
        q_s[h] = query
        k_s[h] = jnp.concatenate([k_of, jnp.zeros_like(k_of)], 1)
        v_s[h] = vg[:, 2 * h * DV : (2 * h + 1) * DV]
        double = jnp.concatenate([query, query], 1)
        spread_q = jnp.where(own_row, jnp.concatenate([double] * (part // 2), 1), 0.0).astype(BF16)
        both = jnp.dot(spread_q, halves[h], preferred_element_type=F32)
        reads.append(both[:, :DV] + both[:, DV:])
    sides = []
    for h in range(2):
        v_of = v_s[h]
        q_k = jnp.sum(q_s[h] * k_s[h][:, :DK], -1, keepdims=True)
        read = keep2[h][0:1, :] * reads[h] + q_k * v_of
        centred = read - jnp.mean(read, -1, keepdims=True)
        normed = centred * lax.rsqrt(jnp.mean(centred * centred, -1, keepdims=True) + EPSILON)
        gate_pre = vg[:, (2 * h + 1) * DV : (2 * h + 2) * DV]
        sides.append((gate_pre * jax.nn.sigmoid(gate_pre) * normed).astype(BF16))
    mixed = jnp.concatenate(sides, 1)
    loaded(8, wo2.at[part_of(c, 128), :])
    arrived(wo2.at[part_of(o, 128), :], wdr.at[3])
    for d in z_order[::-1] + [0]:
        cols = pl.ds(pl.multiple_of(up_z(d) * 256, 256), 256)
        made = jnp.dot(mixed, wo2[:, cols], preferred_element_type=F32).astype(BF16)
        for p in range(2):
            at = 2 * up_z(d) + p
            ps[at] = made[:, p * 128 : (p + 1) * 128]
            copy = remote(ps.at[at], pr.at[c, d], p3s.at[0], p3r.at[0], ep, at)
            if d:
                go(copy)
            else:
                pl.when(c != p)(copy.start)
    pr[c, 0] = ps[tp]
    swap(3, 5, k_s.at[o], kv_in.at[0])
    swap(3, 5, v_s.at[o], kv_in.at[1])
    swap(2, 6, edown, wd2.at[mine, :])
    arrived(kv_in, wdr.at[5])
    k_all[part_of(c, part), :] = k_s[c]
    k_all[part_of(o, part), :] = kv_in[0]
    out[:, 256:384] = jnp.concatenate([k_all[...].T[:DK, :], jnp.zeros((DK, 128 - rows), F32)], 1)
    out[part_of(c, part), 128:256] = v_s[c]
    out[part_of(o, part), 128:256] = kv_in[1]
    load(11, out.at[:, 128:384], out_hbm.at[:, 128:384])
    arrived(ps.at[0 : 2 * nz - 1], p3r.at[0])
    for p in range(2):
        total = tok_own[p * part : (p + 1) * part, :].astype(F32)
        for d in range(nz):
            total += pr[p, d].astype(F32)
        resz[z, p * part : (p + 1) * part, :] = total.astype(BF16)
    p4 = {}
    for d in z_order:
        p4[d] = go(remote(resz.at[z], resz.at[z], p4s.at[0], p4r.at[d], ep, 2 * up_z(d) + c))
    cuts = sorted({min(i, nz) for i in CUTS})
    for g in range(len(cuts) - 1):
        for i in range(cuts[g], cuts[g + 1]):
            if i:
                p4[order[i]].wait_recv()
            rows_out = jnp.dot(picked, resz[down_z(order[i])], preferred_element_type=F32).astype(BF16)
            for e in range(n_ep):
                sel[e, i] = rows_out[e * SLOT : e * SLOT + cap, :]
        span = slice(cuts[g], cuts[g + 1])
        for d in ep_order[::-1]:
            e = up_ep(d)
            remote(
                sel.at[e, span], x2.at[c, d // 2, span], p5s.at[0], p5r.at[g], e, 2 * z + d % 2
            ).start()

        @pl.when(c == 1)
        def _():
            remote(sel.at[ep, span], x2.at[1, 0, span], p5s.at[0], p5r.at[g], ep, 2 * z).start()

        @pl.when(c == 0)
        def _():
            x2[0, 0, span] = sel[ep, span]

    loaded(9, wgu.at[0 : 2 * hid_rows, :])
    arrived(wgu.at[0 : 2 * hid_rows, :], wdr.at[4])
    joins = {min(i, nz) for i in JOINS}
    first_join, wide = True, []
    for i in range(nz):
        if i in cuts:
            g = cuts.index(i)
            span = slice(cuts[g], cuts[g + 1])
            pl.when(c == 1)(functools.partial(arrived, sel.at[:, span], p5r.at[g]))
            pl.when(c == 0)(functools.partial(arrived, sel.at[0 : n_ep - 1, span], p5r.at[g]))
        at = down_z(order[i])
        gains = [nmoe_v[pl.ds(2 * at + p, 1), :] for p in range(2)]
        for s in range(slots):
            span = slice(s * SLOT, s * SLOT + cap)
            both = [x2[p, s, i].astype(F32) for p in range(2)]
            sq[span, :] += both[0] * both[0] + both[1] * both[1]
            for p in range(2):
                lane = (2 * len(wide) + p) * 128
                xg[span, lane : lane + 128] = (both[p] * gains[p]).astype(BF16)
        wide.append(wgu[:, pl.ds(pl.multiple_of(at * 256, 256), 256)])
        if i + 1 in joins:
            used = len(wide) * 256
            more = lax.dot_general(
                xg[:, :used], jnp.concatenate(wide, 1), dims, preferred_element_type=F32
            )
            if first_join:
                acc[...] = more
            elif i + 1 < nz:
                acc[...] += more
            first_join, wide = False, []
    scale = lax.rsqrt(jnp.sum(sq[...], -1, keepdims=True) / (2 * half) + EPSILON)
    gate_part = (acc[:, : 2 * hid_rows] + more[:, : 2 * hid_rows]) * scale
    up_part = (acc[:, 2 * hid_rows :] + more[:, 2 * hid_rows :]) * scale
    hidden = (gate_part * jax.nn.sigmoid(gate_part) * up_part).astype(BF16)
    loaded(10, wd2.at[mine, :])
    arrived(wd2.at[mine, :], wdr.at[6])
    back = z_order[::-1] + [0]
    backs = sorted({min(i, nz) for i in BACK_CUTS})
    far_slots = sorted(range(slots), key=lambda s: (-max(hops(2 * s), hops(2 * s + 1)), s))
    for g in range(len(backs) - 1):
        for i in range(backs[g], backs[g + 1]):
            cols = pl.ds(pl.multiple_of(up_z(back[i]) * 256, 256), 256)
            down = jnp.dot(hidden, wd2[:, cols], preferred_element_type=F32).astype(BF16)
            for s in range(slots):
                for p in range(2):
                    ds[s, p, i] = down[s * SLOT : s * SLOT + cap, p * 128 : (p + 1) * 128]
        span = slice(backs[g], backs[g + 1])
        for s, p in [(s, (p + g) % 2) for s in far_slots[g:] + far_slots[:g] for p in range(2)]:
            if True:
                home = remote(
                    ds.at[s, p, span], ret.at[ep, span], p6s.at[0], p6r.at[g], served(s), 2 * z + p
                )
                if s:
                    home.start()
                    continue
                pl.when(c == 1)(home.start)
                if p == 0:

                    @pl.when(c == 0)
                    def _():
                        ret[ep, span] = ds[0, 0, span]

                else:
                    other = remote(
                        ds.at[s, p, span], ret.at[ep, span], p6s.at[0], p6r.at[g], ep, 2 * z + 1
                    )
                    pl.when(c == 0)(other.start)

    total = resz[z].astype(F32)
    for i in range(nz):
        if i in backs:
            g = backs.index(i)
            span = slice(backs[g], backs[g + 1])
            pl.when(c == 1)(functools.partial(arrived, ret.at[:, span], p6r.at[g]))
            pl.when(c == 0)(functools.partial(arrived, ret.at[0 : n_ep - 1, span], p6r.at[g]))
        for e in range(n_ep):
            flat[e * SLOT : e * SLOT + cap, :] = ret[e, i]
        both = jnp.dot(spread2, flat[...], preferred_element_type=F32)
        weighed = both[:rows, :] + both[rows:, :]
        t = back[i]
        if t:
            qs[t] = weighed.astype(BF16)
            go(remote(qs.at[t], qr.at[t], p7s.at[0], p7r.at[0], ep, 2 * up_z(t) + c))
        else:
            total += weighed
    arrived(qr.at[1:nz], p7r.at[0])
    for d in z_order:
        total += qr[d].astype(F32)
    out[:, :128] = total.astype(BF16).astype(F32)
    load(11, out.at[:, 0:128], out_hbm.at[:, 0:128])
    left(ps.at[0 : 2 * nz - 1], p1s.at[0])
    left(ps.at[0 : 2 * nz - 1], p3s.at[0])
    left(resz.at[1:nz], p4s.at[0])
    left(qs.at[1:nz], p7s.at[0])
    left(keep2.at[0], wds.at[0])
    left(wvg_v.at[0 : 3 * half // 2, :], wds.at[1])
    left(prior_v.at[0], wds.at[4])
    left(wo2.at[part_of(c, 128), :], wds.at[5])
    left(wgu.at[0 : 3 * hid_rows, :], wds.at[2])
    left(kv_in, wds.at[3])
    for ref, sem in ((sel, p5s), (ds, p6s)):
        pl.when(c == 1)(functools.partial(left, ref, sem.at[0]))
        pl.when(c == 0)(functools.partial(left, sel.at[0 : n_ep - 1], sem.at[0]))
    loaded(11, out)


def state_kernel(decay, made, prior, hidden_out, state_out, hidden, state, sems):
    pieces = 16
    size = state.shape[0] // pieces
    hidden[...] = made[:, :128].astype(BF16)
    first = pltpu.make_async_copy(hidden, hidden_out, sems.at[0])
    first.start()
    keep = 1.0 - decay[0]
    for j in range(pieces):
        for row in range(j * size, (j + 1) * size):
            key, value = made[:, 256 + row : 257 + row], made[row : row + 1, 128:256]
            state[row] = keep * prior[row] + key * value
        span = slice(j * size, (j + 1) * size)
        pltpu.make_async_copy(state.at[span], state_out.at[span], sems.at[1]).start()
    first.wait()
    pltpu.make_async_copy(state, state_out, sems.at[1]).wait()


def on_device(
    nx, ny, nz,
    tokens, prior_state, decay_rate, norm_in, query_weight, key_weight, value_weight,
    gate_weight, out_weight, norm_moe, routes, route_weight, expert_gate, expert_up, expert_down,
):
    rows = tokens.shape[0]
    n_ep = nx * ny
    width = SLOT * n_ep
    half = nz * 128
    full = 2 * half
    ffe = expert_gate.shape[2]
    cap = (3 * routes.shape[1] * rows + 2 * n_ep - 1) // (2 * n_ep)
    hbm = pl.BlockSpec(memory_space=pltpu.HBM)
    vmem = pl.BlockSpec(memory_space=pltpu.VMEM)
    part = rows // 2
    scratch = [
        pltpu.VMEM((rows, 384), F32),
        pltpu.SMEM((1,), F32),
        pltpu.VMEM((rows, 128), BF16),
        pltpu.VMEM((2 * nz, part, 128), BF16),
        pltpu.VMEM((2, 2 * DK, full), BF16),
        pltpu.VMEM((full, 4 * DV), BF16),
        pltpu.VMEM((2, part, DK, DV), F32),
        pltpu.VMEM((2, 2 * nz, 128), F32),
        pltpu.VMEM((2, 128), jnp.int32),
        pltpu.VMEM((2, 128), F32),
        pltpu.VMEM((2, 8, 128), F32),
        pltpu.VMEM((2, part * DK, 2 * DV), BF16),
        pltpu.VMEM((2, part, DK), F32),
        pltpu.VMEM((2, part, 2 * DK), F32),
        pltpu.VMEM((2, part, DV), F32),
        pltpu.VMEM((2, part, DV), F32),
        pltpu.VMEM((rows, 2 * DK), F32),
        pltpu.VMEM((2 * DV, full), BF16),
        pltpu.VMEM((2 * nz, part, 128), BF16),
        pltpu.VMEM((2, nz, part, 128), BF16),
        pltpu.VMEM((nz, rows, 128), BF16),
        pltpu.VMEM((n_ep, nz, cap, 128), BF16),
        pltpu.VMEM((2, n_ep // 2, nz, cap, 128), BF16),
        pltpu.VMEM((width // 2, 1024), BF16),
        pltpu.VMEM((width // 2, 128), F32),
        pltpu.VMEM((width // 2, 4 * ffe), F32),
        pltpu.VMEM((4 * ffe, full), BF16),
        pltpu.VMEM((2 * ffe, full), BF16),
        pltpu.VMEM((n_ep // 2, 2, nz, cap, 128), BF16),
        pltpu.VMEM((n_ep, nz, cap, 128), BF16),
        pltpu.VMEM((width, 128), BF16),
        pltpu.VMEM((nz, rows, 128), BF16),
        pltpu.VMEM((nz, rows, 128), BF16),
    ]
    for n in (12, 1, nz, 6, 7, 1, 1, 1, 1, nz, 1, 1):
        scratch.append(pltpu.SemaphoreType.DMA((n,)))
    made = pl.pallas_call(
        functools.partial(layer_kernel, nx, ny, nz, cap),
        out_shape=jax.ShapeDtypeStruct((rows, 384), F32),
        in_specs=[hbm] * 15,
        out_specs=hbm,
        scratch_shapes=scratch,
        compiler_params=pltpu.CompilerParams(
            collective_id=0, has_side_effects=True, vmem_limit_bytes=64000000
        ),
        name="layer",
    )(
        tokens, prior_state.reshape(rows, DK, DV), decay_rate, norm_in.reshape(2 * nz, 128),
        query_weight.T, key_weight.T, value_weight, gate_weight, out_weight,
        norm_moe.reshape(2 * nz, 128), routes.T, route_weight.T,
        expert_gate.reshape(full, ffe).T, expert_up.reshape(full, ffe).T, expert_down.reshape(ffe, full),
    )
    next_hidden, new_state = pl.pallas_call(
        state_kernel,
        out_shape=(jax.ShapeDtypeStruct((rows, 128), BF16), jax.ShapeDtypeStruct((rows, DK, DV), F32)),
        in_specs=[pl.BlockSpec(memory_space=pltpu.SMEM), vmem, vmem],
        out_specs=(hbm, hbm),
        scratch_shapes=[
            pltpu.VMEM((rows, 128), BF16),
            pltpu.VMEM((rows, DK, DV), F32),
            pltpu.SemaphoreType.DMA((2,)),
        ],
        compiler_params=pltpu.CompilerParams(vmem_limit_bytes=16 * 1024 * 1024),
        name="state",
    )(decay_rate, made, prior_state.reshape(rows, DK, DV))
    return (next_hidden, new_state[:, None])


def solution(mesh):
    n_ep, n_tp = mesh.shape["ep"], mesh.shape["tp"]
    nx = next(i for i in range(1, n_ep + 1) if i * i >= n_ep)
    placed = (
        P("ep", "tp"),
        P("ep", "tp", None, None),
        P("tp"),
        P(),
        P(None, "tp"),
        P(None, "tp"),
        P(None, "tp"),
        P(None, "tp"),
        P("tp", None),
        P(),
        P(),
        P(),
        P("ep", None, "tp"),
        P("ep", None, "tp"),
        P("ep", "tp", None),
    )
    return jax.shard_map(
        functools.partial(on_device, nx, n_ep // nx, n_tp // 2),
        mesh=mesh,
        in_specs=placed,
        out_specs=(P("ep", "tp"), P("ep", "tp", None, None)),
        check_vma=False,
    )
```
